128 devices in a mesh: fs: 16 (over z, y), tp: 8 (over x, core).
Axes of the slice: x: 4, y: 4, z: 4, core: 2. Of those that a mesh axis runs over, the one named last changes fastest.
Arguments:
- tokens: bfloat16 [32, 384, 2048], P('fs', None, 'tp'), may hold values from -34 to 34
- mix_gain: float32 [2048], replicated, may hold values from 0.1 to 1.9
- w_bgate: float32 [2048, 2048], P('fs', 'tp'), may hold values from -0.125 to 0.125
- w_cgate: float32 [2048, 2048], P('fs', 'tp'), may hold values from -0.125 to 0.125
- w_value: float32 [2048, 2048], P('fs', 'tp'), may hold values from -0.125 to 0.125
- in_scale: float32 [3, 2048], P(None, 'tp'), may hold values from 0.5 to 2
- mix_taps: float32 [3, 2048], P(None, 'tp'), may hold values from -3.5 to 3.5
- w_mixout: float32 [2048, 2048], P('tp', 'fs'), may hold values from -0.125 to 0.125
- mixout_scale: float32 [1, 2048], P(None, 'fs'), may hold values from 0.5 to 2
- ffn_gain: float32 [2048], replicated, may hold values from 0.1 to 1.9
- w_upgate: float32 [2048, 5632], P('fs', 'tp'), may hold values from -0.125 to 0.125
- w_upval: float32 [2048, 5632], P('fs', 'tp'), may hold values from -0.125 to 0.125
- up_scale: float32 [2, 5632], P(None, 'tp'), may hold values from 0.5 to 2
- ffn_taps: float32 [2, 3, 5632], P(None, None, 'tp'), may hold values from -3.5 to 3.5
- w_down: float32 [5632, 2048], P('tp', 'fs'), may hold values from -0.078125 to 0.078125
- down_scale: float32 [1, 2048], P(None, 'fs'), may hold values from 0.5 to 2
Outputs:
- layer_out: bfloat16 [32, 384, 2048], P('fs', None, 'tp')
The draws below stay inside these ranges and needn't reach their ends.
All inputs are finite; a program needn't handle non-finite values.
Results may differ from the reference program's by a relative error of at most 0.015.
Values may be sent and summed in bfloat16 or wider, within the bound.
A program may use at most 64 MiB of HBM per device.

```python
import math
import jax
import jax.numpy as jnp
from jax import lax

D = 2048
FF = 5632
CONV = 3
LEN = 384
SEQS = 32
N_TP = 8


def draw_tokens(key, part):
    key_base, key_rows, key_cols = jax.random.split(key, 3)
    base = jax.random.normal(key_base, (SEQS, LEN, D), jnp.float32)
    base = jnp.clip(base, -4.0, 4.0)
    row_scale = jnp.exp(jax.random.uniform(key_rows, (SEQS, LEN, 1), jnp.float32, math.log(0.3), math.log(3.0)))
    rising = jnp.exp(math.log(4.0) * (jnp.arange(D, dtype=jnp.float32) / D - 0.5))
    col_scale = rising * jax.random.uniform(key_cols, (D,), jnp.float32, 0.7, 1.4)
    return (base * row_scale * col_scale).astype(jnp.bfloat16)


def block_levels(own_key, shape, cuts, smallest, high):
    factor_of, own = 1.0, jax.random.fold_in(own_key, 6)
    for position, shards_of in cuts:
        draws = jnp.exp(jax.random.uniform(jax.random.fold_in(own, position), (shards_of,), jnp.float32, smallest / len(cuts), high / len(cuts)))
        factor_of = factor_of * jnp.repeat(draws, shape[position] // shards_of).reshape([-1 if axis == position else 1 for axis in range(len(shape))])
    return factor_of


def gaussian(rng, shape, spread, most, cuts=(), kind=jnp.bfloat16):
    loudness = block_levels(rng, shape, cuts, -0.22, 0.18) if cuts else 1.0
    drawn = jax.random.normal(rng, shape, jnp.float32) * spread * loudness
    return jnp.minimum(jnp.maximum(drawn, -most), most).astype(kind)


def setup_inputs(seed: int = 0) -> dict:
    streams_of = jax.random.split(jax.random.key(seed), 17)
    return {
        "tokens": draw_tokens(jax.random.fold_in(streams_of[16], 71), 0),
        "mix_gain": jnp.clip(1.0 + 0.18 * jax.random.normal(streams_of[1], (D,), jnp.float32), 0.1, 1.9),
        "w_bgate": gaussian(streams_of[2], (D, D), D ** -0.5, 0.125, ((0, 16), (1, 8)), jnp.float32),
        "w_cgate": gaussian(streams_of[3], (D, D), D ** -0.5, 0.125, ((0, 16), (1, 8)), jnp.float32),
        "w_value": gaussian(streams_of[4], (D, D), D ** -0.5, 0.125, ((0, 16), (1, 8)), jnp.float32),
        "in_scale": jnp.clip(jnp.exp(math.log(2.0) - 1.3862944 * jax.random.uniform(streams_of[5], (3, D), jnp.float32) ** block_levels(streams_of[5], (3, D), ((1, 8),), -0.2, 0.2)), 0.5, 2.0),
        "mix_taps": gaussian(streams_of[6], (CONV, D), CONV ** -0.5, 3.5, ((1, 8),), jnp.float32),
        "w_mixout": gaussian(streams_of[7], (D, D), D ** -0.5, 0.125, ((0, 8), (1, 16)), jnp.float32),
        "mixout_scale": jnp.clip(jnp.exp(math.log(2.0) - 1.3862944 * jax.random.uniform(streams_of[8], (1, D), jnp.float32) ** block_levels(streams_of[8], (1, D), ((1, 16),), -0.2, 0.2)), 0.5, 2.0),
        "ffn_gain": jnp.clip(1.0 + 0.18 * jax.random.normal(streams_of[9], (D,), jnp.float32), 0.1, 1.9),
        "w_upgate": gaussian(streams_of[10], (D, FF), D ** -0.5, 0.125, ((0, 16), (1, 8)), jnp.float32),
        "w_upval": gaussian(streams_of[11], (D, FF), D ** -0.5, 0.125, ((0, 16), (1, 8)), jnp.float32),
        "up_scale": jnp.clip(jnp.exp(math.log(2.0) - 1.3862944 * jax.random.uniform(streams_of[12], (2, FF), jnp.float32) ** block_levels(streams_of[12], (2, FF), ((1, 8),), -0.2, 0.2)), 0.5, 2.0),
        "ffn_taps": gaussian(streams_of[13], (2, CONV, FF), CONV ** -0.5, 3.5, ((2, 8),), jnp.float32),
        "w_down": gaussian(streams_of[14], (FF, D), FF ** -0.5, 0.078125, ((0, 8), (1, 16)), jnp.float32),
        "down_scale": jnp.clip(jnp.exp(math.log(2.0) - 1.3862944 * jax.random.uniform(streams_of[15], (1, D), jnp.float32) ** block_levels(streams_of[15], (1, D), ((1, 16),), -0.2, 0.2)), 0.5, 2.0),
    }


EPS = 1e-06

def normed_rows(values, gain):
    floats = values.astype(jnp.float32)
    factor = lax.rsqrt(lax.optimization_barrier(jnp.mean(floats * floats, axis=-1, keepdims=True)) + EPS)
    return (floats * factor * gain).astype(jnp.bfloat16).reshape(SEQS * LEN, D)

def causal_taps(values, taps):
    padded = jnp.pad(values, ((0, 0), (CONV - 1, 0), (0, 0)))
    result = jnp.zeros(values.shape, jnp.float32)
    for offset in range(CONV):
        result = result + padded[:, offset:offset + LEN] * taps[offset]
    return result

def project(inputs, matrix, scale):
    return jnp.dot(inputs, matrix.astype(jnp.bfloat16), preferred_element_type=jnp.float32) * scale

def blocked_sum(inputs, matrix, scale):
    inner_width = inputs.shape[1] // N_TP
    total = jnp.zeros((inputs.shape[0], matrix.shape[1]), jnp.float32)
    for block in range(N_TP):
        lower = block * inner_width
        part_out = jnp.dot(inputs[:, lower:lower + inner_width], matrix[lower:lower + inner_width].astype(jnp.bfloat16), preferred_element_type=jnp.float32) * scale
        rounded = lax.optimization_barrier(part_out.astype(jnp.bfloat16))
        total = total + rounded.astype(jnp.float32)
    return total

def reference(tokens, mix_gain, w_bgate, w_cgate, w_value, in_scale, mix_taps, w_mixout, mixout_scale, ffn_gain, w_upgate, w_upval, up_scale, ffn_taps, w_down, down_scale):
    row_count = SEQS * LEN
    normed = normed_rows(tokens, mix_gain)
    bgate = project(normed, w_bgate, in_scale[0])
    cgate = project(normed, w_cgate, in_scale[1])
    value = project(normed, w_value, in_scale[2])
    inner = (cgate * value).reshape(SEQS, LEN, D)
    convolved = causal_taps(inner, mix_taps)
    gated = (bgate.reshape(SEQS, LEN, D) * convolved).astype(jnp.bfloat16).reshape(row_count, D)
    mix = blocked_sum(gated, w_mixout, mixout_scale)
    resid = (tokens.reshape(row_count, D).astype(jnp.float32) + mix).astype(jnp.bfloat16)
    normed_ffn = normed_rows(resid.reshape(SEQS, LEN, D), ffn_gain)
    gate_pre = project(normed_ffn, w_upgate, up_scale[0]).reshape(SEQS, LEN, FF)
    val_pre = project(normed_ffn, w_upval, up_scale[1]).reshape(SEQS, LEN, FF)
    gate_conv = causal_taps(gate_pre, ffn_taps[0])
    val_conv = causal_taps(val_pre, ffn_taps[1])
    active = (jax.nn.silu(gate_conv) * val_conv).astype(jnp.bfloat16).reshape(row_count, FF)
    ffn = blocked_sum(active, w_down, down_scale)
    layer_out = (resid.astype(jnp.float32) + ffn).astype(jnp.bfloat16)
    return layer_out.reshape(SEQS, LEN, D)
```

```python
import functools

import jax
import jax.numpy as jnp
from jax import lax
from jax.experimental import pallas as pl
from jax.experimental.pallas import tpu as pltpu
from jax.sharding import PartitionSpec as P

EPS = 1e-06
BF = jnp.bfloat16
F32 = jnp.float32
SEQ = 384
HALF = SEQ // 2
D = 2048
W = 256
ROUNDS = 13


def kernel(
    tok, mgain, wb, wc, wv, insc, mtaps, wm, msc, fgain, wug, wuv, upsc, ftaps, wd, dsc,
    out,
    g_in, g_mo, g_up, g_ul, g_dn, g_dl,
    tfull, rfull, cbuf, gated, active, tfac, rfac,
    sb, rb, keep, fbuf, nbuf, rf, rn,
    y_send, y_recv, a_send, a_recv, r_send, r_recv,
):
    fs = lax.axis_index("fs")
    tp = lax.axis_index("tp")
    z, y = fs // 4, fs % 4
    x, core = tp // 2, tp % 2
    xp, xm, xf = (x + 1) % 4, (x + 3) % 4, (x + 2) % 4
    dev_xp = (fs, xp * 2 + core)
    dev_xm = (fs, xm * 2 + core)
    dev_sib = (fs, x * 2 + 1 - core)
    dev_axis = (
        ((z * 4 + (y + 1) % 4, tp), (z * 4 + (y + 3) % 4, tp)),
        ((((z + 1) % 4) * 4 + y, tp), (((z + 3) % 4) * 4 + y, tp)),
    )
    pos = (y, z)
    started = []

    def send(src, dst, ssem, rsem, dev):
        copy = pltpu.make_async_remote_copy(
            src_ref=src, dst_ref=dst, send_sem=ssem, recv_sem=rsem,
            device_id=dev, device_id_type=pl.DeviceIdType.MESH,
        )
        copy.start()
        started.append(copy)

    def arrived(dst, rsem):
        pltpu.make_async_copy(dst, dst, rsem).wait()

    barrier = pltpu.get_barrier_semaphore()
    for dev in (*dev_axis[0], *dev_axis[1], dev_xp, dev_xm, dev_sib):
        pl.semaphore_signal(barrier, inc=1, device_id=dev, device_id_type=pl.DeviceIdType.MESH)

    def rounded(w):
        return w.astype(BF).astype(F32)

    def column(gain):
        return jnp.broadcast_to(gain[pl.ds(fs, 1), :], (128, 128)).T

    mcol = column(mgain)
    mcol2 = jnp.concatenate([mcol, mcol], axis=1)
    for k, (w, row) in enumerate(((wc, 1), (wv, 2), (wb, 0))):
        g_in[k, z, y] = (rounded(w[...]) * mcol2 * insc[row : row + 1, :]).astype(BF)
    g_mo[0, z, y] = (rounded(wm[...]) * msc[...]).astype(BF)
    fcol = column(fgain)
    for j in range(5):
        cols = slice(128 * j, 128 * j + 128)
        g_up[j, z, y, :, 0:128] = (rounded(wug[:, cols]) * fcol * upsc[0:1, cols]).astype(BF)
        g_up[j, z, y, :, 128:256] = (rounded(wuv[:, cols]) * fcol * upsc[1:2, cols]).astype(BF)
    tail = slice(640, 704)
    g_ul[0, z, y] = (
        jnp.concatenate(
            [rounded(wug[:, tail]) * upsc[0:1, tail], rounded(wuv[:, tail]) * upsc[1:2, tail]], axis=1
        )
        * fcol
    ).astype(BF)
    for k in range(2):
        g_dn[k, z, y] = (rounded(wd[256 * k : 256 * k + 256, :]) * dsc[...]).astype(BF)
    g_dl[0, z, y] = (rounded(wd[512:704, :]) * dsc[...]).astype(BF)

    pl.semaphore_wait(barrier, 7)

    rounds = (
        [(g_in, k, 128) for k in range(3)]
        + [(g_mo, 0, 256)]
        + [(g_up, k, 128) for k in range(5)]
        + [(g_ul, 0, 128)]
        + [(g_dn, k, 256) for k in range(2)]
        + [(g_dl, 0, 192)]
    )

    def block(r, h, p_at, q_at, lo, n):
        ref, k, rows = rounds[r]
        zz, yy = (q_at, p_at) if h == 0 else (p_at, q_at)
        return ref.at[k, zz, yy, pl.ds(lo, n), :]

    def line(r, h, q_at, lo, n):
        ref, k, rows = rounds[r]
        if h == 0:
            return ref.at[k, q_at, pl.ds(0, 4), pl.ds(lo, n), :]
        return ref.at[k, pl.ds(0, 4), q_at, pl.ds(lo, n), :]

    def geometry(r, h):
        half = rounds[r][2] // 2
        lo = half * h
        return lo, half, lo, lo + half // 2, half // 2, pos[h], pos[1 - h]

    def s1(r):
        if not 0 <= r < ROUNDS:
            return
        for h in range(2):
            lo, half, up, dn, quarter, p, q = geometry(r, h)
            own = block(r, h, p, q, lo, half)
            for d in range(2):
                send(own, own, y_send.at[r, h, d], y_recv.at[r, h, d], dev_axis[h][d])

    def s2(r):
        if not 0 <= r < ROUNDS:
            return
        for h in range(2):
            lo, half, up, dn, quarter, p, q = geometry(r, h)
            for d, at, part in ((0, (p + 3) % 4, up), (1, (p + 1) % 4, dn)):
                arrived(block(r, h, at, q, lo, half), y_recv.at[r, h, d])
                piece = block(r, h, at, q, part, quarter)
                send(piece, piece, y_send.at[r, h, 2 + d], y_recv.at[r, h, 2 + d], dev_axis[h][d])

    def s3(r):
        if not 0 <= r < ROUNDS:
            return
        for h in range(2):
            lo, half, up, dn, quarter, p, q = geometry(r, h)
            for d, part in ((0, up), (1, dn)):
                arrived(block(r, h, (p + 2) % 4, q, part, quarter), y_recv.at[r, h, 2 + d])
            row = line(r, h, q, lo, half)
            for d in range(2):
                send(row, row, y_send.at[r, h, 4 + d], y_recv.at[r, h, 4 + d], dev_axis[1 - h][d])

    def s4(r):
        if not 0 <= r < ROUNDS:
            return
        for h in range(2):
            lo, half, up, dn, quarter, p, q = geometry(r, h)
            for d, at, part in ((0, (q + 3) % 4, up), (1, (q + 1) % 4, dn)):
                arrived(line(r, h, at, lo, half), y_recv.at[r, h, 4 + d])
                piece = line(r, h, at, part, quarter)
                send(piece, piece, y_send.at[r, h, 6 + d], y_recv.at[r, h, 6 + d], dev_axis[1 - h][d])

    def done(r):
        for h in range(2):
            lo, half, up, dn, quarter, p, q = geometry(r, h)
            for d, part in ((0, up), (1, dn)):
                arrived(line(r, h, (q + 2) % 4, part, quarter), y_recv.at[r, h, 6 + d])

    def tick(k):
        s1(k + 2)
        s2(k + 1)
        s3(k)
        s4(k - 1)

    def cols_of(xx, cc):
        return pl.ds(pl.multiple_of((xx * 2 + cc) * W, W), W)

    def gather_own(u, buf, s, src):
        dst = buf.at[s, :, cols_of(x, core)]
        send(src, dst, a_send.at[u, 0], a_recv.at[u, 0], dev_xp)
        send(src, dst, a_send.at[u, 1], a_recv.at[u, 1], dev_xm)
        send(src, dst, a_send.at[u, 2], a_recv.at[u, 4], dev_sib)

    def gather_near(u, buf, s):
        for d, xx, lo, dev in ((0, xm, 0, dev_xp), (1, xp, HALF, dev_xm)):
            whole = buf.at[s, :, cols_of(xx, core)]
            arrived(whole, a_recv.at[u, d])
            piece = buf.at[s, pl.ds(lo, HALF), cols_of(xx, core)]
            send(piece, piece, a_send.at[u, 3 + d], a_recv.at[u, 2 + d], dev)
            send(whole, whole, a_send.at[u, 5 + d], a_recv.at[u, 5 + d], dev_sib)

    def gather_far(u, buf, s):
        for d, lo in ((0, 0), (1, HALF)):
            arrived(buf.at[s, pl.ds(lo, HALF), cols_of(xf, core)], a_recv.at[u, 2 + d])
        whole = buf.at[s, :, cols_of(xf, core)]
        send(whole, whole, a_send.at[u, 7], a_recv.at[u, 7], dev_sib)

    def gather_done(u, buf, s):
        for k, xx in ((4, x), (5, xm), (6, xp), (7, xf)):
            arrived(buf.at[s, :, cols_of(xx, 1 - core)], a_recv.at[u, k])

    def row_factor(buf, fac, s):
        total = jnp.zeros((SEQ, 128), F32)
        for j in range(D // 128):
            v = buf[s, :, 128 * j : 128 * j + 128].astype(F32)
            total = total + v * v
        mean = jnp.sum(total, axis=1, keepdims=True) * (1.0 / D)
        fac[s] = jnp.broadcast_to(lax.rsqrt(mean + EPS), (SEQ, 128))

    def shifted(v, n):
        row = lax.broadcasted_iota(jnp.int32, v.shape, 0)
        return jnp.where(row >= n, pltpu.roll(v, n, 0), 0.0)

    def causal(v, taps):
        return shifted(v, 2) * taps[0:1] + shifted(v, 1) * taps[1:2] + v * taps[2:3]

    def wide(fac, s):
        f = fac[s]
        return jnp.concatenate([f, f], axis=1)

    order = (xf, xp, xm, x)

    def scatter_parts(u, part):
        for k, xx in enumerate(order):
            sb[u, k] = part(xx, 1 - core).astype(BF)
            send(sb.at[u, k], rb.at[u, k], r_send.at[u, k], r_recv.at[u, k], dev_sib)
            keep[u, k] = part(xx, core)

    def scatter_far(u):
        arrived(rb.at[u, 0], r_recv.at[u, 0])
        fbuf[u] = (keep[u, 0] + rb[u, 0].astype(F32)).astype(BF)
        for d, dev in ((0, dev_xp), (1, dev_xm)):
            send(
                fbuf.at[u, pl.ds(HALF * d, HALF)], rf.at[u, d],
                r_send.at[u, 4 + d], r_recv.at[u, 4 + d], dev,
            )

    def scatter_near(u):
        for d, dev in ((0, dev_xp), (1, dev_xm)):
            arrived(rb.at[u, 1 + d], r_recv.at[u, 1 + d])
            lo = HALF * (1 - d)
            nbuf[u, d, lo : lo + HALF] = (
                keep[u, 1 + d, lo : lo + HALF] + rb[u, 1 + d, lo : lo + HALF].astype(F32)
            ).astype(BF)
            rows = pl.ds(lo, HALF)
            send(nbuf.at[u, d, rows], rn.at[u, d, rows], r_send.at[u, 6 + d], r_recv.at[u, 6 + d], dev)

    def scatter_last(u):
        for d, dev in ((0, dev_xp), (1, dev_xm)):
            arrived(rf.at[u, d], r_recv.at[u, 4 + d])
            lo = HALF * d
            nbuf[u, d, lo : lo + HALF] = (
                keep[u, 1 + d, lo : lo + HALF]
                + rb[u, 1 + d, lo : lo + HALF].astype(F32)
                + rf[u, d].astype(F32)
            ).astype(BF)
            rows = pl.ds(lo, HALF)
            send(nbuf.at[u, d, rows], rn.at[u, d, rows], r_send.at[u, 8 + d], r_recv.at[u, 8 + d], dev)

    def scatter_total(u):
        arrived(rb.at[u, 3], r_recv.at[u, 3])
        for d in range(2):
            for k, lo in ((6, HALF * (1 - d)), (8, HALF * d)):
                arrived(rn.at[u, d, pl.ds(lo, HALF)], r_recv.at[u, k + d])
        return keep[u, 3] + rb[u, 3].astype(F32) + rn[u, 0].astype(F32) + rn[u, 1].astype(F32)

    def dot(a, b):
        return jnp.dot(a, b, preferred_element_type=F32)

    def in_cgate():
        @pl.loop(0, 2)
        def _(s):
            cbuf[s] = dot(tfull[s], g_in[0].reshape(D, W))

    def in_value():
        @pl.loop(0, 2)
        def _(s):
            f = wide(tfac, s)
            inner = dot(tfull[s], g_in[1].reshape(D, W)) * cbuf[s] * (f * f)
            cbuf[s] = causal(inner, mtaps) * f

    def in_bgate():
        @pl.loop(0, 2)
        def _(s):
            gated[s] = (dot(tfull[s], g_in[2].reshape(D, W)) * cbuf[s]).astype(BF)

    def mix_part(s):
        def part(xx, cc):
            mat = jnp.concatenate([g_mo[0, xx, 2 * cc], g_mo[0, xx, 2 * cc + 1]], axis=1)
            return dot(gated[s], mat)

        return part

    def up(s):
        @pl.loop(0, 5)
        def _(j):
            cols = pl.ds(pl.multiple_of(128 * j, 128), 128)
            pre = dot(rfull[s], g_up[j].reshape(D, W)) * wide(rfac, s)
            taps = jnp.concatenate([ftaps[0, :, cols], ftaps[1, :, cols]], axis=1)
            conv = causal(pre, taps)
            gate, val = conv[:, 0:128], conv[:, 128:256]
            active[s, :, cols] = (gate / (1.0 + jnp.exp(-gate)) * val).astype(BF)

        pre = dot(rfull[s], g_ul[0].reshape(D, 128)) * rfac[s]
        taps = jnp.concatenate([ftaps[0, :, tail], ftaps[1, :, tail]], axis=1)
        conv = causal(pre, taps)
        act = conv / (1.0 + jnp.exp(-conv)) * pltpu.roll(conv, 64, 1)
        active[s, :, 640:704] = act[:, 0:64].astype(BF)

    def down_part(s):
        def part(xx, cc):
            total = None
            for ref, k, lo, n in ((g_dn, 0, 0, 256), (g_dn, 1, 256, 256), (g_dl, 0, 512, 192)):
                mat = jnp.concatenate([ref[k, xx, 2 * cc], ref[k, xx, 2 * cc + 1]], axis=1)
                term = dot(active[s, :, lo : lo + n], mat)
                total = term if total is None else total + term
            return total

        return part

    own = cols_of(x, core)

    s1(0)
    for s in range(2):
        gather_own(s, tfull, s, tok.at[s])
    s1(1)
    for s in range(2):
        tfull[s, :, own] = tok[s]
    s2(0)
    tick(0)
    gather_near(0, tfull, 0)
    tick(1)
    gather_near(1, tfull, 1)
    gather_far(0, tfull, 0)
    tick(2)
    gather_far(1, tfull, 1)
    for s in range(2):
        gather_done(s, tfull, s)
        row_factor(tfull, tfac, s)
    done(0)
    in_cgate()
    tick(3)
    done(1)
    in_value()
    tick(4)
    done(2)
    in_bgate()
    tick(5)
    done(3)
    scatter_parts(0, mix_part(0))
    scatter_far(0)
    scatter_near(0)
    scatter_parts(1, mix_part(1))
    scatter_far(1)
    scatter_near(1)
    tick(6)
    scatter_last(0)
    scatter_last(1)
    tick(7)

    def residual(s):
        rfull[s, :, own] = (tok[s].astype(F32) + scatter_total(s)).astype(BF)
        gather_own(2 + s, rfull, s, rfull.at[s, :, own])

    residual(0)
    tick(8)
    residual(1)
    tick(9)
    gather_near(2, rfull, 0)
    gather_near(3, rfull, 1)
    tick(10)
    gather_far(2, rfull, 0)
    gather_far(3, rfull, 1)
    tick(11)
    for r in range(4, 10):
        done(r)
    for s in range(2):
        gather_done(2 + s, rfull, s)
        row_factor(rfull, rfac, s)
        up(s)
        if s == 0:
            tick(12)
            tick(13)
    for r in range(10, 13):
        done(r)
    for s in range(2):
        scatter_parts(2 + s, down_part(s))
        scatter_far(2 + s)
        scatter_near(2 + s)
    for s in range(2):
        scatter_last(2 + s)
    for s in range(2):
        out[s] = (rfull[s, :, own].astype(F32) + scatter_total(2 + s)).astype(BF)
    for copy in started:
        copy.wait_send()


def on_device(
    tokens, mix_gain, w_bgate, w_cgate, w_value, in_scale, mix_taps, w_mixout, mixout_scale,
    ffn_gain, w_upgate, w_upval, up_scale, ffn_taps, w_down, down_scale,
):
    args = (
        tokens, mix_gain.reshape(16, 128), w_bgate, w_cgate, w_value, in_scale, mix_taps, w_mixout,
        mixout_scale, ffn_gain.reshape(16, 128), w_upgate, w_upval, up_scale, ffn_taps, w_down, down_scale,
    )
    vmem = pltpu.VMEM
    dma = pltpu.SemaphoreType.DMA
    return pl.pallas_call(
        kernel,
        out_shape=jax.ShapeDtypeStruct(tokens.shape, BF),
        in_specs=[pl.BlockSpec(memory_space=pltpu.VMEM)] * len(args),
        out_specs=pl.BlockSpec(memory_space=pltpu.VMEM),
        scratch_shapes=[
            vmem((3, 4, 4, 128, W), BF),
            vmem((1, 4, 4, 256, 128), BF),
            vmem((5, 4, 4, 128, W), BF),
            vmem((1, 4, 4, 128, 128), BF),
            vmem((2, 4, 4, 256, 128), BF),
            vmem((1, 4, 4, 192, 128), BF),
            vmem((2, SEQ, D), BF),
            vmem((2, SEQ, D), BF),
            vmem((2, SEQ, W), F32),
            vmem((2, SEQ, W), BF),
            vmem((2, SEQ, 704), BF),
            vmem((2, SEQ, 128), F32),
            vmem((2, SEQ, 128), F32),
            vmem((4, 4, SEQ, W), BF),
            vmem((4, 4, SEQ, W), BF),
            vmem((4, 4, SEQ, W), F32),
            vmem((4, SEQ, W), BF),
            vmem((4, 2, SEQ, W), BF),
            vmem((4, 2, HALF, W), BF),
            vmem((4, 2, SEQ, W), BF),
            dma((ROUNDS, 2, 8)),
            dma((ROUNDS, 2, 8)),
            dma((4, 8)),
            dma((4, 8)),
            dma((4, 10)),
            dma((4, 10)),
        ],
        compiler_params=pltpu.CompilerParams(
            collective_id=0, has_side_effects=True, vmem_limit_bytes=62 * 1024 * 1024
        ),
        name="layer",
    )(*args)


def solution(mesh):
    return jax.shard_map(
        on_device,
        mesh=mesh,
        in_specs=(
            P("fs", None, "tp"),
            P(),
            P("fs", "tp"),
            P("fs", "tp"),
            P("fs", "tp"),
            P(None, "tp"),
            P(None, "tp"),
            P("tp", "fs"),
            P(None, "fs"),
            P(),
            P("fs", "tp"),
            P("fs", "tp"),
            P(None, "tp"),
            P(None, None, "tp"),
            P("tp", "fs"),
            P(None, "fs"),
        ),
        out_specs=P("fs", None, "tp"),
        check_vma=False,
    )
```

```python
import functools

import jax
import jax.numpy as jnp
from jax import lax
from jax.experimental import pallas as pl
from jax.experimental.pallas import tpu as pltpu
from jax.sharding import PartitionSpec as P

EPS = 1e-06
BF = jnp.bfloat16
F32 = jnp.float32
SEQ = 384
HALF = SEQ // 2
D = 2048
W = 256
ROUNDS = 13


def kernel(
    tok, mgain, wb, wc, wv, insc, mtaps, wm, msc, fgain, wug, wuv, upsc, ftaps, wd, dsc,
    out,
    g_in, g_mo, g_up, g_ul, g_dn, g_dl,
    tfull, rfull, cbuf, gated, active, tfac, rfac,
    sb, rb, keep, fbuf, nbuf, rf, rn,
    y_send, y_recv, a_send, a_recv, r_send, r_recv,
):
    fs = lax.axis_index("fs")
    tp = lax.axis_index("tp")
    z, y = fs // 4, fs % 4
    x, core = tp // 2, tp % 2
    xp, xm, xf = (x + 1) % 4, (x + 3) % 4, (x + 2) % 4
    dev_xp = (fs, xp * 2 + core)
    dev_xm = (fs, xm * 2 + core)
    dev_sib = (fs, x * 2 + 1 - core)
    dev_axis = (
        ((z * 4 + (y + 1) % 4, tp), (z * 4 + (y + 3) % 4, tp)),
        ((((z + 1) % 4) * 4 + y, tp), (((z + 3) % 4) * 4 + y, tp)),
    )
    pos = (y, z)
    sent = []

    def push(src, dst, ssem, rsem, dev):
        pltpu.make_async_remote_copy(
            src_ref=src, dst_ref=dst, send_sem=ssem, recv_sem=rsem,
            device_id=dev, device_id_type=pl.DeviceIdType.MESH,
        ).start()

    def send(src, dst, ssem, rsem, dev):
        push(src, dst, ssem, rsem, dev)
        sent.append((src, ssem))

    def arrived(dst, rsem):
        pltpu.make_async_copy(dst, dst, rsem).wait()

    barrier = pltpu.get_barrier_semaphore()
    for dev in (*dev_axis[0], *dev_axis[1], dev_xp, dev_xm, dev_sib):
        pl.semaphore_signal(barrier, inc=1, device_id=dev, device_id_type=pl.DeviceIdType.MESH)

    def rounded(w):
        return w.astype(BF).astype(F32)

    def column(gain):
        return jnp.broadcast_to(gain[pl.ds(fs, 1), :], (128, 128)).T

    mcol = column(mgain)
    mcol2 = jnp.concatenate([mcol, mcol], axis=1)
    for k, (w, row) in enumerate(((wc, 1), (wv, 2), (wb, 0))):
        g_in[k, z, y] = (rounded(w[...]) * mcol2 * insc[row : row + 1, :]).astype(BF)
    g_mo[0, z, y] = (rounded(wm[...]) * msc[...]).astype(BF)
    frow = fgain[pl.ds(fs, 1), :]
    for j in range(5):
        cols = slice(128 * j, 128 * j + 128)
        for k, w in enumerate((wug, wuv)):
            g_up[j, z, y, :, 128 * k : 128 * k + 128] = (
                (rounded(w[cols, :]) * frow).T * upsc[k : k + 1, cols]
            ).astype(BF)
    tail = slice(640, 704)
    both = rounded(jnp.concatenate([wug[tail, :], wuv[tail, :]], axis=0))
    tail_scale = jnp.concatenate([upsc[0:1, tail], upsc[1:2, tail]], axis=1)
    g_ul[0, z, y] = ((both * frow).T * tail_scale).astype(BF)
    for k in range(2):
        g_dn[k, z, y] = (rounded(wd[256 * k : 256 * k + 256, :]) * dsc[...]).astype(BF)
    g_dl[0, z, y] = (rounded(wd[512:704, :]) * dsc[...]).astype(BF)

    pl.semaphore_wait(barrier, 7)

    rounds = (
        [(g_in, k, 128) for k in range(3)]
        + [(g_mo, 0, 256)]
        + [(g_up, k, 128) for k in range(5)]
        + [(g_ul, 0, 128)]
        + [(g_dn, k, 256) for k in range(2)]
        + [(g_dl, 0, 192)]
    )

    def block(r, h, p_at, q_at, lo, n):
        ref, k, rows = rounds[r]
        zz, yy = (q_at, p_at) if h == 0 else (p_at, q_at)
        return ref.at[k, zz, yy, pl.ds(lo, n), :]

    def line(r, h, q_at, lo, n):
        ref, k, rows = rounds[r]
        if h == 0:
            return ref.at[k, q_at, pl.ds(0, 4), pl.ds(lo, n), :]
        return ref.at[k, pl.ds(0, 4), q_at, pl.ds(lo, n), :]

    def geometry(r, h):
        half = rounds[r][2] // 2
        lo = half * h
        return lo, half, lo, lo + half // 2, half // 2, pos[h], pos[1 - h]

    def s1(r):
        if not 0 <= r < ROUNDS:
            return
        for h in range(2):
            lo, half, up, dn, quarter, p, q = geometry(r, h)
            own = block(r, h, p, q, lo, half)
            for d in range(2):
                send(own, own, y_send.at[r, h, d], y_recv.at[r, h, d], dev_axis[h][d])
            across(r, h, p)

    def across(r, h, p_at):
        lo, half, up, dn, quarter, p, q = geometry(r, h)
        piece = block(r, h, p_at, q, lo, half)
        for d in range(2):
            push(piece, piece, y_send.at[r, h, 4 + d], y_recv.at[r, h, 4 + d], dev_axis[1 - h][d])

    def s2(r):
        if not 0 <= r < ROUNDS:
            return
        for h in range(2):
            lo, half, up, dn, quarter, p, q = geometry(r, h)
            for d, at, part in ((0, (p + 3) % 4, up), (1, (p + 1) % 4, dn)):
                arrived(block(r, h, at, q, lo, half), y_recv.at[r, h, d])
                piece = block(r, h, at, q, part, quarter)
                send(piece, piece, y_send.at[r, h, 2 + d], y_recv.at[r, h, 2 + d], dev_axis[h][d])
                across(r, h, at)

    def s3(r):
        if not 0 <= r < ROUNDS:
            return
        for h in range(2):
            lo, half, up, dn, quarter, p, q = geometry(r, h)
            for d, part in ((0, up), (1, dn)):
                arrived(block(r, h, (p + 2) % 4, q, part, quarter), y_recv.at[r, h, 2 + d])
            across(r, h, (p + 2) % 4)
            for d in range(2):
                sent.append((line(r, h, q, lo, half), y_send.at[r, h, 4 + d]))

    def s4(r):
        if not 0 <= r < ROUNDS:
            return
        for h in range(2):
            lo, half, up, dn, quarter, p, q = geometry(r, h)
            for d, at, part in ((0, (q + 3) % 4, up), (1, (q + 1) % 4, dn)):
                arrived(line(r, h, at, lo, half), y_recv.at[r, h, 4 + d])
                for k in range(4):
                    piece = block(r, h, k, at, part, quarter)
                    push(piece, piece, y_send.at[r, h, 6 + d], y_recv.at[r, h, 6 + d], dev_axis[1 - h][d])
                sent.append((line(r, h, at, part, quarter), y_send.at[r, h, 6 + d]))

    def done(r):
        for h in range(2):
            lo, half, up, dn, quarter, p, q = geometry(r, h)
            for d, part in ((0, up), (1, dn)):
                arrived(line(r, h, (q + 2) % 4, part, quarter), y_recv.at[r, h, 6 + d])

    def tick(k):
        s1(k + 2)
        s2(k + 1)
        s3(k)
        s4(k - 1)

    def cols_of(xx, cc):
        return pl.ds(pl.multiple_of((xx * 2 + cc) * W, W), W)

    def gather_own(u, buf, s, src):
        dst = buf.at[s, :, cols_of(x, core)]
        send(src, dst, a_send.at[u, 0], a_recv.at[u, 0], dev_xp)
        send(src, dst, a_send.at[u, 1], a_recv.at[u, 1], dev_xm)
        send(src, dst, a_send.at[u, 2], a_recv.at[u, 4], dev_sib)

    def gather_near(u, buf, s):
        for d, xx, lo, dev in ((0, xm, 0, dev_xp), (1, xp, HALF, dev_xm)):
            whole = buf.at[s, :, cols_of(xx, core)]
            arrived(whole, a_recv.at[u, d])
            piece = buf.at[s, pl.ds(lo, HALF), cols_of(xx, core)]
            send(piece, piece, a_send.at[u, 3 + d], a_recv.at[u, 2 + d], dev)
            send(whole, whole, a_send.at[u, 5 + d], a_recv.at[u, 5 + d], dev_sib)

    def gather_far(u, buf, s):
        for d, lo in ((0, 0), (1, HALF)):
            arrived(buf.at[s, pl.ds(lo, HALF), cols_of(xf, core)], a_recv.at[u, 2 + d])
        whole = buf.at[s, :, cols_of(xf, core)]
        send(whole, whole, a_send.at[u, 7], a_recv.at[u, 7], dev_sib)

    def gather_done(u, buf, s):
        for k, xx in ((4, x), (5, xm), (6, xp), (7, xf)):
            arrived(buf.at[s, :, cols_of(xx, 1 - core)], a_recv.at[u, k])

    def row_factor(buf, fac, s):
        total = jnp.zeros((SEQ, 128), F32)
        for j in range(D // 128):
            v = buf[s, :, 128 * j : 128 * j + 128].astype(F32)
            total = total + v * v
        mean = jnp.sum(total, axis=1, keepdims=True) * (1.0 / D)
        fac[s] = jnp.broadcast_to(lax.rsqrt(mean + EPS), (SEQ, 128))

    def shifted(v, n):
        row = lax.broadcasted_iota(jnp.int32, v.shape, 0)
        return jnp.where(row >= n, pltpu.roll(v, n, 0), 0.0)

    def causal(v, taps):
        return shifted(v, 2) * taps[0:1] + shifted(v, 1) * taps[1:2] + v * taps[2:3]

    def wide(fac, s):
        f = fac[s]
        return jnp.concatenate([f, f], axis=1)

    order = (xf, xp, xm, x)

    def scatter_parts(u, part):
        for k, xx in enumerate(order):
            sb[u, k] = part(xx, 1 - core).astype(BF)
            send(sb.at[u, k], rb.at[u, k], r_send.at[u, k], r_recv.at[u, k], dev_sib)
            keep[u, k] = part(xx, core)

    def scatter_far(u):
        arrived(rb.at[u, 0], r_recv.at[u, 0])
        fbuf[u] = (keep[u, 0] + rb[u, 0].astype(F32)).astype(BF)
        for d, dev in ((0, dev_xp), (1, dev_xm)):
            send(
                fbuf.at[u, pl.ds(HALF * d, HALF)], rf.at[u, d],
                r_send.at[u, 4 + d], r_recv.at[u, 4 + d], dev,
            )

    def scatter_near(u):
        for d, dev in ((0, dev_xp), (1, dev_xm)):
            arrived(rb.at[u, 1 + d], r_recv.at[u, 1 + d])
            lo = HALF * (1 - d)
            nbuf[u, d, lo : lo + HALF] = (
                keep[u, 1 + d, lo : lo + HALF] + rb[u, 1 + d, lo : lo + HALF].astype(F32)
            ).astype(BF)
            rows = pl.ds(lo, HALF)
            send(nbuf.at[u, d, rows], rn.at[u, d, rows], r_send.at[u, 6 + d], r_recv.at[u, 6 + d], dev)

    def scatter_last(u):
        for d, dev in ((0, dev_xp), (1, dev_xm)):
            arrived(rf.at[u, d], r_recv.at[u, 4 + d])
            lo = HALF * d
            nbuf[u, d, lo : lo + HALF] = (
                keep[u, 1 + d, lo : lo + HALF]
                + rb[u, 1 + d, lo : lo + HALF].astype(F32)
                + rf[u, d].astype(F32)
            ).astype(BF)
            rows = pl.ds(lo, HALF)
            send(nbuf.at[u, d, rows], rn.at[u, d, rows], r_send.at[u, 8 + d], r_recv.at[u, 8 + d], dev)

    def scatter_total(u):
        arrived(rb.at[u, 3], r_recv.at[u, 3])
        for d in range(2):
            for k, lo in ((6, HALF * (1 - d)), (8, HALF * d)):
                arrived(rn.at[u, d, pl.ds(lo, HALF)], r_recv.at[u, k + d])
        return keep[u, 3] + rb[u, 3].astype(F32) + rn[u, 0].astype(F32) + rn[u, 1].astype(F32)

    def dot(a, b):
        return jnp.dot(a, b, preferred_element_type=F32)

    def in_cgate():
        @pl.loop(0, 2)
        def _(s):
            cbuf[s] = dot(tfull[s], g_in[0].reshape(D, W))

    def in_value():
        @pl.loop(0, 2)
        def _(s):
            f = wide(tfac, s)
            inner = dot(tfull[s], g_in[1].reshape(D, W)) * cbuf[s] * (f * f)
            cbuf[s] = causal(inner, mtaps) * f

    def in_bgate():
        @pl.loop(0, 2)
        def _(s):
            gated[s] = (dot(tfull[s], g_in[2].reshape(D, W)) * cbuf[s]).astype(BF)

    def mix_part(s):
        def part(xx, cc):
            mat = jnp.concatenate([g_mo[0, xx, 2 * cc], g_mo[0, xx, 2 * cc + 1]], axis=1)
            return dot(gated[s], mat)

        return part

    def up(s):
        @pl.loop(0, 5)
        def _(j):
            cols = pl.ds(pl.multiple_of(128 * j, 128), 128)
            pre = dot(rfull[s], g_up[j].reshape(D, W)) * wide(rfac, s)
            taps = jnp.concatenate([ftaps[:, 0, cols], ftaps[:, 1, cols]], axis=1)
            conv = causal(pre, taps)
            gate, val = conv[:, 0:128], conv[:, 128:256]
            active[s, :, cols] = (gate / (1.0 + jnp.exp(-gate)) * val).astype(BF)

        pre = dot(rfull[s], g_ul[0].reshape(D, 128)) * rfac[s]
        taps = jnp.concatenate([ftaps[:, 0, tail], ftaps[:, 1, tail]], axis=1)
        conv = causal(pre, taps)
        act = conv / (1.0 + jnp.exp(-conv)) * pltpu.roll(conv, 64, 1)
        active[s, :, 640:704] = act[:, 0:64].astype(BF)

    def down_part(s):
        def part(xx, cc):
            total = None
            for ref, k, lo, n in ((g_dn, 0, 0, 256), (g_dn, 1, 256, 256), (g_dl, 0, 512, 192)):
                mat = jnp.concatenate([ref[k, xx, 2 * cc], ref[k, xx, 2 * cc + 1]], axis=1)
                term = dot(active[s, :, lo : lo + n], mat)
                total = term if total is None else total + term
            return total

        return part

    own = cols_of(x, core)

    s1(0)
    for s in range(2):
        gather_own(s, tfull, s, tok.at[s])
    s1(1)
    for s in range(2):
        tfull[s, :, own] = tok[s]
    s2(0)
    tick(0)
    gather_near(0, tfull, 0)
    tick(1)
    gather_near(1, tfull, 1)
    gather_far(0, tfull, 0)
    tick(2)
    gather_far(1, tfull, 1)
    for s in range(2):
        gather_done(s, tfull, s)
        row_factor(tfull, tfac, s)
    done(0)
    in_cgate()
    tick(3)
    done(1)
    in_value()
    tick(4)
    done(2)
    in_bgate()
    tick(5)
    done(3)
    scatter_parts(0, mix_part(0))
    scatter_far(0)
    scatter_near(0)
    scatter_parts(1, mix_part(1))
    scatter_far(1)
    tick(6)
    scatter_last(0)
    scatter_near(1)
    scatter_last(1)
    tick(7)

    def residual(s):
        rfull[s, :, own] = (tok[s].astype(F32) + scatter_total(s)).astype(BF)
        gather_own(2 + s, rfull, s, rfull.at[s, :, own])

    residual(0)
    tick(8)
    residual(1)
    gather_near(2, rfull, 0)
    tick(9)
    gather_near(3, rfull, 1)
    tick(10)
    gather_far(2, rfull, 0)
    gather_far(3, rfull, 1)
    tick(11)
    for r in range(4, 10):
        done(r)
    for s in range(2):
        gather_done(2 + s, rfull, s)
        row_factor(rfull, rfac, s)
        up(s)
        if s == 0:
            tick(12)
            tick(13)
    for r in range(10, 13):
        done(r)
    scatter_parts(2, down_part(0))
    scatter_far(2)
    scatter_near(2)
    scatter_parts(3, down_part(1))
    scatter_far(3)
    scatter_last(2)
    scatter_near(3)
    scatter_last(3)
    for s in range(2):
        out[s] = (rfull[s, :, own].astype(F32) + scatter_total(2 + s)).astype(BF)
    for src, ssem in sent:
        arrived(src, ssem)


def on_device(
    tokens, mix_gain, w_bgate, w_cgate, w_value, in_scale, mix_taps, w_mixout, mixout_scale,
    ffn_gain, w_upgate, w_upval, up_scale, ffn_taps, w_down, down_scale,
):
    args = (
        tokens, mix_gain.reshape(16, 128), w_bgate, w_cgate, w_value, in_scale, mix_taps, w_mixout,
        mixout_scale, ffn_gain.reshape(16, 128), w_upgate.T, w_upval.T, up_scale,
        jnp.swapaxes(ffn_taps, 0, 1), w_down, down_scale,
    )
    vmem = pltpu.VMEM
    dma = pltpu.SemaphoreType.DMA
    return pl.pallas_call(
        kernel,
        out_shape=jax.ShapeDtypeStruct(tokens.shape, BF),
        in_specs=[pl.BlockSpec(memory_space=pltpu.VMEM)] * len(args),
        out_specs=pl.BlockSpec(memory_space=pltpu.VMEM),
        scratch_shapes=[
            vmem((3, 4, 4, 128, W), BF),
            vmem((1, 4, 4, 256, 128), BF),
            vmem((5, 4, 4, 128, W), BF),
            vmem((1, 4, 4, 128, 128), BF),
            vmem((2, 4, 4, 256, 128), BF),
            vmem((1, 4, 4, 192, 128), BF),
            vmem((2, SEQ, D), BF),
            vmem((2, SEQ, D), BF),
            vmem((2, SEQ, W), F32),
            vmem((2, SEQ, W), BF),
            vmem((2, SEQ, 704), BF),
            vmem((2, SEQ, 128), F32),
            vmem((2, SEQ, 128), F32),
            vmem((4, 4, SEQ, W), BF),
            vmem((4, 4, SEQ, W), BF),
            vmem((4, 4, SEQ, W), F32),
            vmem((4, SEQ, W), BF),
            vmem((4, 2, SEQ, W), BF),
            vmem((4, 2, HALF, W), BF),
            vmem((4, 2, SEQ, W), BF),
            dma((ROUNDS, 2, 8)),
            dma((ROUNDS, 2, 8)),
            dma((4, 8)),
            dma((4, 8)),
            dma((4, 10)),
            dma((4, 10)),
        ],
        compiler_params=pltpu.CompilerParams(
            collective_id=0, has_side_effects=True, vmem_limit_bytes=62 * 1024 * 1024
        ),
        name="layer",
    )(*args)


def solution(mesh):
    return jax.shard_map(
        on_device,
        mesh=mesh,
        in_specs=(
            P("fs", None, "tp"),
            P(),
            P("fs", "tp"),
            P("fs", "tp"),
            P("fs", "tp"),
            P(None, "tp"),
            P(None, "tp"),
            P("tp", "fs"),
            P(None, "fs"),
            P(),
            P("fs", "tp"),
            P("fs", "tp"),
            P(None, "tp"),
            P(None, None, "tp"),
            P("tp", "fs"),
            P(None, "fs"),
        ),
        out_specs=P("fs", None, "tp"),
        check_vma=False,
    )
```

```python
import functools

import jax
import jax.numpy as jnp
from jax import lax
from jax.experimental import pallas as pl
from jax.experimental.pallas import tpu as pltpu
from jax.sharding import PartitionSpec as P

EPS = 1e-06
BF = jnp.bfloat16
F32 = jnp.float32
SEQ = 384
HALF = SEQ // 2
D = 2048
W = 256
ROUNDS = 13


def kernel(
    tok_h, mgain_h, wb_h, wc_h, wv_h, insc_h, mtaps_h, wm_h, msc_h, fgain_h, wug_h, wuv_h, upsc_h, ftaps_h,
    wd_h, dsc_h,
    out,
    mgain, wb, wc, wv, insc, mtaps, wm, msc, fgain, wug, wuv, upsc, ftaps, wd, dsc,
    g_in, g_mo, g_up, g_ul, g_dt, g_d,
    tfull, rfull, cbuf, gated, active, fac, squares, acc, acc_tail,
    sb, rb, keep, fbuf, nbuf, rf, rn,
    sb2, rb2, keep2, fbuf2, nbuf2, rf2, rn2,
    y_send, y_recv, a_send, a_recv, r_send, r_recv, load_sem,
):
    fs = lax.axis_index("fs")
    tp = lax.axis_index("tp")
    z, y = fs // 4, fs % 4
    x, core = tp // 2, tp % 2
    xp, xm, xf = (x + 1) % 4, (x + 3) % 4, (x + 2) % 4
    dev_xp = (fs, xp * 2 + core)
    dev_xm = (fs, xm * 2 + core)
    dev_sib = (fs, x * 2 + 1 - core)
    dev_axis = (
        ((z * 4 + (y + 1) % 4, tp), (z * 4 + (y + 3) % 4, tp)),
        ((((z + 1) % 4) * 4 + y, tp), (((z + 3) % 4) * 4 + y, tp)),
    )
    pos = (y, z)
    sent = []

    def push(src, dst, ssem, rsem, dev):
        pltpu.make_async_remote_copy(
            src_ref=src, dst_ref=dst, send_sem=ssem, recv_sem=rsem,
            device_id=dev, device_id_type=pl.DeviceIdType.MESH,
        ).start()

    def send(src, dst, ssem, rsem, dev):
        push(src, dst, ssem, rsem, dev)
        sent.append((src, ssem))

    def arrived(dst, rsem):
        pltpu.make_async_copy(dst, dst, rsem).wait()

    barrier = pltpu.get_barrier_semaphore()
    for dev in (*dev_axis[0], *dev_axis[1], dev_xp, dev_xm, dev_sib):
        pl.semaphore_signal(barrier, inc=1, device_id=dev, device_id_type=pl.DeviceIdType.MESH)

    loads = {}

    def load(name, src, dst):
        loads[name] = pltpu.make_async_copy(src, dst, load_sem.at[len(loads)])
        loads[name].start()

    def cols_of(xx, cc):
        return pl.ds(pl.multiple_of((xx * 2 + cc) * W, W), W)

    for s in range(2):
        load(("tok", s), tok_h.at[s], tfull.at[s, :, cols_of(x, core)])
    for name, src, dst in (
        ("mgain", mgain_h, mgain), ("insc", insc_h, insc), ("wc", wc_h, wc), ("wv", wv_h, wv), ("wb", wb_h, wb),
        ("msc", msc_h, msc), ("wm", wm_h, wm), ("fgain", fgain_h, fgain), ("upsc", upsc_h, upsc),
        ("wug", wug_h, wug), ("wuv", wuv_h, wuv), ("dsc", dsc_h, dsc), ("wd", wd_h, wd),
        ("mtaps", mtaps_h, mtaps), ("ftaps", ftaps_h, ftaps),
    ):
        load(name, src, dst)

    def ready(*names):
        for name in names:
            if name in loads:
                loads.pop(name).wait()

    def rounded(w):
        return w.astype(BF).astype(F32)

    tail = slice(640, 704)

    def pack(r):
        if r < 3:
            w, row = ((wc, 1), (wv, 2), (wb, 0))[r]
            ready("mgain", "insc", ("wc", "wv", "wb")[r])
            col = jnp.broadcast_to(mgain[pl.ds(fs, 1), :], (128, 128)).T
            col = jnp.concatenate([col, col], axis=1)
            g_in[r, z, y] = (rounded(w[...]) * col * insc[row : row + 1, :]).astype(BF)
        elif r == 3:
            ready("msc", "wm")
            g_mo[0, z, y] = (rounded(wm[...]) * msc[...]).astype(BF)
        elif r < 9:
            ready("fgain", "upsc", "wug", "wuv")
            frow = fgain[pl.ds(fs, 1), :]
            j = r - 4
            cols = slice(128 * j, 128 * j + 128)
            for k, w in enumerate((wug, wuv)):
                g_up[j, z, y, :, 128 * k : 128 * k + 128] = (
                    (rounded(w[cols, :]) * frow).T * upsc[k : k + 1, cols]
                ).astype(BF)
        elif r == 9:
            frow = fgain[pl.ds(fs, 1), :]
            both = rounded(jnp.concatenate([wug[tail, :], wuv[tail, :]], axis=0))
            tail_scale = jnp.concatenate([upsc[0:1, tail], upsc[1:2, tail]], axis=1)
            g_ul[0, z, y] = ((both * frow).T * tail_scale).astype(BF)
        elif r == 10:
            ready("dsc", "wd")
            last = rounded(wd[tail, :]) * dsc[...]
            turned = jnp.concatenate([last, last], axis=0).T
            lane = lax.broadcasted_iota(jnp.int32, (64, 128), 1)
            g_dt[0, z, y] = jnp.where(lane < 64, turned[0:64], turned[64:128]).astype(BF)
        elif r < 13:
            lo = 64 * (r - 11)
            for j in range(5):
                cols = slice(128 * j, 128 * j + 128)
                turned = (rounded(wd[cols, :]) * dsc[...]).T
                g_d[r - 11, z, y, :, cols] = turned[lo : lo + 64].astype(BF)

    rounds = (
        [(g_in, k, 128) for k in range(3)]
        + [(g_mo, 0, 256)]
        + [(g_up, k, 128) for k in range(5)]
        + [(g_ul, 0, 128), (g_dt, 0, 64)]
        + [(g_d, k, 64) for k in range(2)]
    )

    def block(r, h, p_at, q_at, lo, n):
        ref, k, rows = rounds[r]
        zz, yy = (q_at, p_at) if h == 0 else (p_at, q_at)
        return ref.at[k, zz, yy, pl.ds(lo, n), :]

    def line(r, h, q_at, lo, n):
        ref, k, rows = rounds[r]
        if h == 0:
            return ref.at[k, q_at, pl.ds(0, 4), pl.ds(lo, n), :]
        return ref.at[k, pl.ds(0, 4), q_at, pl.ds(lo, n), :]

    def geometry(r, h):
        half = rounds[r][2] // 2
        lo = half * h
        return lo, half, lo, lo + half // 2, half // 2, pos[h], pos[1 - h]

    def s1(r):
        if not 0 <= r < ROUNDS:
            return
        pack(r + 1)
        for h in range(2):
            lo, half, up, dn, quarter, p, q = geometry(r, h)
            own = block(r, h, p, q, lo, half)
            for d in range(2):
                send(own, own, y_send.at[r, h, d], y_recv.at[r, h, d], dev_axis[h][d])
            across(r, h, p)

    def across(r, h, p_at):
        lo, half, up, dn, quarter, p, q = geometry(r, h)
        piece = block(r, h, p_at, q, lo, half)
        for d in range(2):
            push(piece, piece, y_send.at[r, h, 4 + d], y_recv.at[r, h, 4 + d], dev_axis[1 - h][d])

    def s2(r):
        if not 0 <= r < ROUNDS:
            return
        for h in range(2):
            lo, half, up, dn, quarter, p, q = geometry(r, h)
            for d, at, part in ((0, (p + 3) % 4, up), (1, (p + 1) % 4, dn)):
                arrived(block(r, h, at, q, lo, half), y_recv.at[r, h, d])
                piece = block(r, h, at, q, part, quarter)
                send(piece, piece, y_send.at[r, h, 2 + d], y_recv.at[r, h, 2 + d], dev_axis[h][d])
                across(r, h, at)

    def s3(r):
        if not 0 <= r < ROUNDS:
            return
        for h in range(2):
            lo, half, up, dn, quarter, p, q = geometry(r, h)
            for d, part in ((0, up), (1, dn)):
                arrived(block(r, h, (p + 2) % 4, q, part, quarter), y_recv.at[r, h, 2 + d])
            across(r, h, (p + 2) % 4)
            for d in range(2):
                sent.append((line(r, h, q, lo, half), y_send.at[r, h, 4 + d]))

    def s4(r):
        if not 0 <= r < ROUNDS:
            return
        for h in range(2):
            lo, half, up, dn, quarter, p, q = geometry(r, h)
            for d, at, part in ((0, (q + 3) % 4, up), (1, (q + 1) % 4, dn)):
                arrived(line(r, h, at, lo, half), y_recv.at[r, h, 4 + d])
                for k in range(4):
                    piece = block(r, h, k, at, part, quarter)
                    push(piece, piece, y_send.at[r, h, 6 + d], y_recv.at[r, h, 6 + d], dev_axis[1 - h][d])
                sent.append((line(r, h, at, part, quarter), y_send.at[r, h, 6 + d]))

    def done(r):
        for h in range(2):
            lo, half, up, dn, quarter, p, q = geometry(r, h)
            for d, part in ((0, up), (1, dn)):
                arrived(line(r, h, (q + 2) % 4, part, quarter), y_recv.at[r, h, 6 + d])

    def ahead(k):
        s1(k + 2)
        s2(k + 1)
        s3(k)

    def tick(k):
        ahead(k)
        s4(k - 1)

    def gather_own(u, buf, s, src):
        dst = buf.at[s, :, cols_of(x, core)]
        send(src, dst, a_send.at[u, 0], a_recv.at[u, 0], dev_xp)
        send(src, dst, a_send.at[u, 1], a_recv.at[u, 1], dev_xm)
        send(src, dst, a_send.at[u, 2], a_recv.at[u, 4], dev_sib)

    def gather_near(u, buf, s):
        for d, xx, lo, dev in ((0, xm, 0, dev_xp), (1, xp, HALF, dev_xm)):
            whole = buf.at[s, :, cols_of(xx, core)]
            arrived(whole, a_recv.at[u, d])
            piece = buf.at[s, pl.ds(lo, HALF), cols_of(xx, core)]
            send(piece, piece, a_send.at[u, 3 + d], a_recv.at[u, 2 + d], dev)
            send(whole, whole, a_send.at[u, 5 + d], a_recv.at[u, 5 + d], dev_sib)

    def gather_far(u, buf, s):
        for d, lo in ((0, 0), (1, HALF)):
            arrived(buf.at[s, pl.ds(lo, HALF), cols_of(xf, core)], a_recv.at[u, 2 + d])
        whole = buf.at[s, :, cols_of(xf, core)]
        send(whole, whole, a_send.at[u, 7], a_recv.at[u, 7], dev_sib)

    def gather_done(u, buf, s):
        for k, xx in ((4, x), (5, xm), (6, xp), (7, xf)):
            arrived(buf.at[s, :, cols_of(xx, 1 - core)], a_recv.at[u, k])

    def wide_cols(xx):
        return pl.ds(pl.multiple_of(xx * 2 * W, 2 * W), 2 * W)

    def add_squares(buf, s, xx, first=False):
        v = buf[s, :, wide_cols(xx)].astype(F32)
        v = v * v
        total = v[:, 0:128] + v[:, 128:256] + v[:, 256:384] + v[:, 384:512]
        squares[s] = total if first else squares[s] + total

    def row_factor(s):
        mean = jnp.sum(squares[s], axis=1, keepdims=True) * (1.0 / D)
        fac[s] = jnp.broadcast_to(lax.rsqrt(mean + EPS), (SEQ, 128))

    def shifted(v, n):
        row = lax.broadcasted_iota(jnp.int32, v.shape, 0)
        return jnp.where(row >= n, pltpu.roll(v, n, 0), 0.0)

    def causal(v, taps):
        return shifted(v, 2) * taps[0:1] + shifted(v, 1) * taps[1:2] + v * taps[2:3]

    def wide(s):
        f = fac[s]
        return jnp.concatenate([f, f], axis=1)

    order = (xf, xp, xm, x)

    class Unit:
        def __init__(self, u, sems, sb, rb, keep, fbuf, nbuf, rf, rn):
            self.sb, self.rb, self.fbuf, self.nbuf, self.rf, self.rn = (
                ref.at[u] for ref in (sb, rb, fbuf, nbuf, rf, rn)
            )
            self.keep = keep
            self.ssem, self.rsem = r_send.at[sems], r_recv.at[sems]

        def part(self, k):
            send(self.sb.at[k], self.rb.at[k], self.ssem.at[k], self.rsem.at[k], dev_sib)

        def both(self, k, d):
            return self.keep(k, d) + self.rb[k, d].astype(F32)

        def far(self):
            arrived(self.rb.at[0], self.rsem.at[0])
            for d, dev in ((0, dev_xp), (1, dev_xm)):
                self.fbuf[d] = self.both(0, d).astype(BF)
            for d, dev in ((0, dev_xp), (1, dev_xm)):
                send(self.fbuf.at[d], self.rf.at[d], self.ssem.at[4 + d], self.rsem.at[4 + d], dev)

        def near(self):
            for d, dev in ((0, dev_xp), (1, dev_xm)):
                arrived(self.rb.at[1 + d], self.rsem.at[1 + d])
                self.nbuf[d, 1 - d] = self.both(1 + d, 1 - d).astype(BF)
            for d, dev in ((0, dev_xp), (1, dev_xm)):
                send(
                    self.nbuf.at[d, 1 - d], self.rn.at[d, 1 - d],
                    self.ssem.at[6 + d], self.rsem.at[6 + d], dev,
                )

        def last(self):
            for d, dev in ((0, dev_xp), (1, dev_xm)):
                arrived(self.rf.at[d], self.rsem.at[4 + d])
                self.nbuf[d, d] = (self.both(1 + d, d) + self.rf[d].astype(F32)).astype(BF)
                send(self.nbuf.at[d, d], self.rn.at[d, d], self.ssem.at[8 + d], self.rsem.at[8 + d], dev)

        def landed(self):
            arrived(self.rb.at[3], self.rsem.at[3])
            for d in range(2):
                arrived(self.rn.at[d, 1 - d], self.rsem.at[6 + d])
                arrived(self.rn.at[d, d], self.rsem.at[8 + d])

        def total(self, d):
            return self.both(3, d) + self.rn[0, d].astype(F32) + self.rn[1, d].astype(F32)

    def mix_unit(s):
        return Unit(s, s, sb, rb, lambda k, d: keep[s, k, d], fbuf, nbuf, rf, rn)

    def ffn_unit(h):
        return Unit(
            h, 2 + h, sb2, rb2, lambda k, d: keep2[h, k, 2 * core + d], fbuf2, nbuf2, rf2, rn2
        )

    def dot(a, b):
        return jnp.dot(a, b, preferred_element_type=F32)

    def in_cgate():
        @pl.loop(0, 2)
        def _(s):
            cbuf[s] = dot(tfull[s], g_in[0].reshape(D, W))

    def in_value():
        @pl.loop(0, 2)
        def _(s):
            f = wide(s)
            inner = dot(tfull[s], g_in[1].reshape(D, W)) * cbuf[s] * (f * f)
            cbuf[s] = causal(inner, mtaps) * f

    def in_bgate():
        @pl.loop(0, 2)
        def _(s):
            gated[s] = (dot(tfull[s], g_in[2].reshape(D, W)) * cbuf[s]).astype(BF)

    def mix_parts(s, unit):
        for k, xx in enumerate(order):
            for cc in (1 - core, core):
                mat = jnp.concatenate([g_mo[0, xx, 2 * cc], g_mo[0, xx, 2 * cc + 1]], axis=1)
                term = dot(gated[s], mat).reshape(2, HALF, W)
                if cc is core:
                    keep[s, k] = term
                else:
                    sb[s, k] = term.astype(BF)
                    unit.part(k)

    def up_dots(s, j, blocks):
        total = None
        for xx in blocks:
            mat = g_ul[0, xx].reshape(512, 128) if j is None else g_up[j, xx].reshape(512, W)
            term = dot(rfull[s, :, wide_cols(xx)], mat)
            total = term if total is None else total + term
        return total

    def up_first(s):
        @pl.loop(0, 5)
        def _(j):
            acc[s, j] = up_dots(s, j, (x, xm, xp))

        acc_tail[s] = up_dots(s, None, (x, xm, xp))

    def silu(v):
        return v / (1.0 + jnp.exp(-v))

    def up_second(s):
        @pl.loop(0, 5)
        def _(j):
            cols = pl.ds(pl.multiple_of(128 * j, 128), 128)
            pre = (acc[s, j] + up_dots(s, j, (xf,))) * wide(s)
            taps = jnp.concatenate([ftaps[:, 0, cols], ftaps[:, 1, cols]], axis=1)
            conv = causal(pre, taps)
            active[s, :, cols] = (silu(conv[:, 0:128]) * conv[:, 128:256]).astype(BF)

        pre = (acc_tail[s] + up_dots(s, None, (xf,))) * fac[s]
        taps = jnp.concatenate([ftaps[:, 0, tail], ftaps[:, 1, tail]], axis=1)
        conv = causal(pre, taps)
        act = silu(conv) * pltpu.roll(conv, 64, 1)
        lane = lax.broadcasted_iota(jnp.int32, (SEQ, 128), 1)
        act = jnp.where(lane < 64, act, 0.0)
        active[s, :, 640:768] = act.astype(BF)
        active[s, :, 768:896] = pltpu.roll(act, 64, 1).astype(BF)

    def turned_dot(a, b):
        return lax.dot_general(a, b, (((1,), (1,)), ((), ())), preferred_element_type=F32)

    def down_parts(h, unit):
        for k, xx in enumerate(order):
            for s in range(2):
                term = turned_dot(g_d[h, xx].reshape(256, 640), active[s, :, 0:640])
                lo = 640 + 128 * h
                term = term + turned_dot(g_dt[0, xx].reshape(256, 128), active[s, :, lo : lo + 128])
                keep2[h, k, :, :, SEQ * s : SEQ * s + SEQ] = term.reshape(4, 64, SEQ)
            sb2[h, k] = keep2[h, k, pl.ds(2 * (1 - core), 2)].astype(BF)
            unit.part(k)

    own = cols_of(x, core)

    ready(("tok", 0), ("tok", 1))
    pl.semaphore_wait(barrier, 7)
    for s in range(2):
        gather_own(s, tfull, s, tfull.at[s, :, own])
    pack(0)
    s1(0)
    s1(1)
    s2(0)
    tick(0)
    gather_near(0, tfull, 0)
    tick(1)
    gather_near(1, tfull, 1)
    gather_far(0, tfull, 0)
    tick(2)
    gather_far(1, tfull, 1)
    ready("mtaps", "ftaps")
    for s in range(2):
        gather_done(s, tfull, s)
        for xx in range(4):
            add_squares(tfull, s, xx, xx == 0)
        row_factor(s)
    ahead(3)
    done(0)
    in_cgate()
    s4(2)
    ahead(4)
    done(1)
    in_value()
    s4(3)
    done(2)
    in_bgate()
    ahead(5)
    done(3)
    u0, u1 = mix_unit(0), mix_unit(1)
    mix_parts(0, u0)
    u0.far()
    u0.near()
    s4(4)
    mix_parts(1, u1)
    u1.far()
    ahead(6)
    u0.last()
    u1.near()
    s4(5)
    u1.last()
    ahead(7)

    def residual(s, unit):
        unit.landed()
        for d in range(2):
            rows = slice(HALF * d, HALF * d + HALF)
            rfull[s, rows, own] = (tfull[s, rows, own].astype(F32) + unit.total(d)).astype(BF)
        gather_own(2 + s, rfull, s, rfull.at[s, :, own])

    residual(0, u0)
    s4(6)
    ahead(8)
    residual(1, u1)
    gather_near(2, rfull, 0)
    s4(7)
    ahead(9)
    for r in range(4, 8):
        done(r)
    gather_near(3, rfull, 1)
    tick(10)

    def near_done(u, buf, s):
        for k, xx in ((4, x), (5, xm), (6, xp)):
            arrived(buf.at[s, :, cols_of(xx, 1 - core)], a_recv.at[u, k])

    def far_done(u, buf, s):
        arrived(buf.at[s, :, cols_of(xf, 1 - core)], a_recv.at[u, 7])

    s4(8)
    tick(11)
    done(8)
    done(9)
    near_done(2, rfull, 0)
    for k, xx in enumerate((x, xm, xp)):
        add_squares(rfull, 0, xx, k == 0)
    up_first(0)
    gather_far(2, rfull, 0)
    tick(12)
    near_done(3, rfull, 1)
    for k, xx in enumerate((x, xm, xp)):
        add_squares(rfull, 1, xx, k == 0)
    up_first(1)
    gather_far(3, rfull, 1)
    tick(13)
    for s in range(2):
        far_done(2 + s, rfull, s)
        add_squares(rfull, s, xf)
        row_factor(s)
        up_second(s)
    done(10)
    done(11)
    v0, v1 = ffn_unit(0), ffn_unit(1)
    down_parts(0, v0)
    v0.far()
    v0.near()
    done(12)
    down_parts(1, v1)
    v1.far()
    v0.last()
    v1.near()
    v1.last()
    total = []
    for h, unit in enumerate((v0, v1)):
        unit.landed()
        total.append([unit.total(d) for d in range(2)])
    for s in range(2):
        for d in range(2):
            lanes = slice(SEQ * s, SEQ * s + SEQ)
            turned = jnp.concatenate([total[0][d][:, lanes], total[1][d][:, lanes]], axis=0).T
            cols = pl.ds(pl.multiple_of((x * 2 + core) * W + 128 * d, 128), 128)
            out[s, :, 128 * d : 128 * d + 128] = (rfull[s, :, cols].astype(F32) + turned).astype(BF)
    for src, ssem in sent:
        arrived(src, ssem)


def on_device(
    tokens, mix_gain, w_bgate, w_cgate, w_value, in_scale, mix_taps, w_mixout, mixout_scale,
    ffn_gain, w_upgate, w_upval, up_scale, ffn_taps, w_down, down_scale,
):
    args = (
        tokens, mix_gain.reshape(16, 128), w_bgate, w_cgate, w_value, in_scale, mix_taps, w_mixout,
        mixout_scale, ffn_gain.reshape(16, 128), w_upgate.T, w_upval.T, up_scale,
        jnp.swapaxes(ffn_taps, 0, 1), w_down, down_scale,
    )
    vmem = pltpu.VMEM

    def exchange_buffers(piece, kept):
        return (
            vmem((2, 4, 2, *piece), BF),
            vmem((2, 4, 2, *piece), BF),
            vmem((2, 4, kept, *piece), F32),
            vmem((2, 2, *piece), BF),
            vmem((2, 2, 2, *piece), BF),
            vmem((2, 2, *piece), BF),
            vmem((2, 2, 2, *piece), BF),
        )

    dma = pltpu.SemaphoreType.DMA
    return pl.pallas_call(
        kernel,
        out_shape=jax.ShapeDtypeStruct(tokens.shape, BF),
        in_specs=[pl.BlockSpec(memory_space=pl.ANY)] * len(args),
        out_specs=pl.BlockSpec(memory_space=pltpu.VMEM),
        scratch_shapes=[
            *(vmem(a.shape, a.dtype) for a in args[1:]),
            vmem((3, 4, 4, 128, W), BF),
            vmem((1, 4, 4, 256, 128), BF),
            vmem((5, 4, 4, 128, W), BF),
            vmem((1, 4, 4, 128, 128), BF),
            vmem((1, 4, 4, 64, 128), BF),
            vmem((2, 4, 4, 64, 640), BF),
            vmem((2, SEQ, D), BF),
            vmem((2, SEQ, D), BF),
            vmem((2, SEQ, W), F32),
            vmem((2, SEQ, W), BF),
            vmem((2, SEQ, 896), BF),
            vmem((2, SEQ, 128), F32),
            vmem((2, SEQ, 128), F32),
            vmem((2, 5, SEQ, W), F32),
            vmem((2, SEQ, 128), F32),
            *exchange_buffers((HALF, W), 2),
            *exchange_buffers((64, 2 * SEQ), 4),
            dma((ROUNDS, 2, 8)),
            dma((ROUNDS, 2, 8)),
            dma((4, 8)),
            dma((4, 8)),
            dma((4, 10)),
            dma((4, 10)),
            dma((17,)),
        ],
        compiler_params=pltpu.CompilerParams(
            collective_id=0, has_side_effects=True, vmem_limit_bytes=62 * 1024 * 1024
        ),
        name="layer",
    )(*args)


def solution(mesh):
    return jax.shard_map(
        on_device,
        mesh=mesh,
        in_specs=(
            P("fs", None, "tp"),
            P(),
            P("fs", "tp"),
            P("fs", "tp"),
            P("fs", "tp"),
            P(None, "tp"),
            P(None, "tp"),
            P("tp", "fs"),
            P(None, "fs"),
            P(),
            P("fs", "tp"),
            P("fs", "tp"),
            P(None, "tp"),
            P(None, None, "tp"),
            P("tp", "fs"),
            P(None, "fs"),
        ),
        out_specs=P("fs", None, "tp"),
        check_vma=False,
    )
```

```python
import functools

import jax
import jax.numpy as jnp
from jax import lax
from jax.experimental import pallas as pl
from jax.experimental.pallas import tpu as pltpu
from jax.sharding import PartitionSpec as P

EPS = 1e-06
BF = jnp.bfloat16
F32 = jnp.float32
SEQ = 384
HALF = SEQ // 2
D = 2048
W = 256
ROUNDS = 13


def kernel(
    tok_h, mgain_h, wb_h, wc_h, wv_h, insc_h, mtaps_h, wm_h, msc_h, fgain_h, wug_h, wuv_h, upsc_h, ftaps_h,
    wd_h, dsc_h,
    out,
    mgain, wb, wc, wv, insc, mtaps, wm, msc, fgain, wug, wuv, upsc, ftaps, wd, dsc,
    g_in, g_mo, g_up, g_ul, g_dt, g_d,
    tfull, rfull, cbuf, gated, active, fac, squares, acc, acc_tail,
    sb, rb, keep, fbuf, nbuf, rf, rn,
    sb2, rb2, keep2, fbuf2, nbuf2, rf2, rn2,
    y_send, y_recv, a_send, a_recv, r_send, r_recv, load_sem,
):
    fs = lax.axis_index("fs")
    tp = lax.axis_index("tp")
    z, y = fs // 4, fs % 4
    x, core = tp // 2, tp % 2
    xp, xm, xf = (x + 1) % 4, (x + 3) % 4, (x + 2) % 4
    dev_xp = (fs, xp * 2 + core)
    dev_xm = (fs, xm * 2 + core)
    dev_sib = (fs, x * 2 + 1 - core)
    dev_axis = (
        ((z * 4 + (y + 1) % 4, tp), (z * 4 + (y + 3) % 4, tp)),
        ((((z + 1) % 4) * 4 + y, tp), (((z + 3) % 4) * 4 + y, tp)),
    )
    pos = (y, z)
    sent = []

    def slot(zz):
        return (zz - x + 5) % 4


    def push(src, dst, ssem, rsem, dev):
        pltpu.make_async_remote_copy(
            src_ref=src, dst_ref=dst, send_sem=ssem, recv_sem=rsem,
            device_id=dev, device_id_type=pl.DeviceIdType.MESH,
        ).start()

    def send(src, dst, ssem, rsem, dev):
        push(src, dst, ssem, rsem, dev)
        sent.append((src, ssem))

    def arrived(dst, rsem):
        pltpu.make_async_copy(dst, dst, rsem).wait()

    barrier = pltpu.get_barrier_semaphore()
    for dev in (*dev_axis[0], *dev_axis[1], dev_xp, dev_xm, dev_sib):
        pl.semaphore_signal(barrier, inc=1, device_id=dev, device_id_type=pl.DeviceIdType.MESH)

    loads = {}

    def load(name, src, dst):
        loads[name] = pltpu.make_async_copy(src, dst, load_sem.at[len(loads)])
        loads[name].start()

    def cols_of(place, cc):
        return pl.ds(pl.multiple_of((place * 2 + cc) * W, W), W)

    for s in range(2):
        load(("tok", s), tok_h.at[s], tfull.at[s, :, cols_of(1, core)])
    for name, src, dst in (
        ("mgain", mgain_h, mgain), ("insc", insc_h, insc), ("wc", wc_h, wc), ("wv", wv_h, wv), ("wb", wb_h, wb),
        ("msc", msc_h, msc), ("wm", wm_h, wm), ("fgain", fgain_h, fgain), ("upsc", upsc_h, upsc),
        ("wug", wug_h, wug), ("wuv", wuv_h, wuv), ("dsc", dsc_h, dsc), ("wd", wd_h, wd),
        ("mtaps", mtaps_h, mtaps), ("ftaps", ftaps_h, ftaps),
    ):
        load(name, src, dst)

    def ready(*names):
        for name in names:
            if name in loads:
                loads.pop(name).wait()

    def rounded(w):
        return w.astype(BF).astype(F32)

    tail = slice(640, 704)

    mine = slot(z)

    def pack(r):
        if r < 3:
            w, row = ((wc, 1), (wv, 2), (wb, 0))[r]
            ready("mgain", "insc", ("wc", "wv", "wb")[r])
            col = jnp.broadcast_to(mgain[pl.ds(fs, 1), :], (128, 128)).T
            col = jnp.concatenate([col, col], axis=1)
            g_in[r, mine, y] = (rounded(w[...]) * col * insc[row : row + 1, :]).astype(BF)
        elif r == 3:
            ready("msc", "wm")
            g_mo[0, mine, y] = (rounded(wm[...]) * msc[...]).astype(BF)
        elif r < 9:
            ready("fgain", "upsc", "wug", "wuv")
            frow = fgain[pl.ds(fs, 1), :]
            j = r - 4
            cols = slice(128 * j, 128 * j + 128)
            for k, w in enumerate((wug, wuv)):
                g_up[j, mine, y, :, 128 * k : 128 * k + 128] = (
                    (rounded(w[cols, :]) * frow).T * upsc[k : k + 1, cols]
                ).astype(BF)
        elif r == 9:
            frow = fgain[pl.ds(fs, 1), :]
            both = rounded(jnp.concatenate([wug[tail, :], wuv[tail, :]], axis=0))
            tail_scale = jnp.concatenate([upsc[0:1, tail], upsc[1:2, tail]], axis=1)
            g_ul[0, mine, y] = ((both * frow).T * tail_scale).astype(BF)
        elif r == 10:
            ready("dsc", "wd")
            last = rounded(wd[tail, :]) * dsc[...]
            turned = jnp.concatenate([last, last], axis=0).T
            lane = lax.broadcasted_iota(jnp.int32, (64, 128), 1)
            g_dt[0, mine, y] = jnp.where(lane < 64, turned[0:64], turned[64:128]).astype(BF)
        elif r < 13:
            lo = 64 * (r - 11)
            for j in range(5):
                cols = slice(128 * j, 128 * j + 128)
                turned = (rounded(wd[cols, :]) * dsc[...]).T
                g_d[r - 11, mine, y, :, cols] = turned[lo : lo + 64].astype(BF)

    rounds = (
        [(g_in, k, 128) for k in range(3)]
        + [(g_mo, 0, 256)]
        + [(g_up, k, 128) for k in range(5)]
        + [(g_ul, 0, 128), (g_dt, 0, 64)]
        + [(g_d, k, 64) for k in range(2)]
    )

    def block(r, h, p_at, q_at, lo, n):
        ref, k, rows = rounds[r]
        zz, yy = (q_at, p_at) if h == 0 else (p_at, q_at)
        return ref.at[k, slot(zz), yy, pl.ds(lo, n), :]

    def line(r, h, q_at, lo, n):
        ref, k, rows = rounds[r]
        if h == 0:
            return ref.at[k, slot(q_at), pl.ds(0, 4), pl.ds(lo, n), :]
        return ref.at[k, pl.ds(0, 4), q_at, pl.ds(lo, n), :]

    def geometry(r, h):
        half = rounds[r][2] // 2
        lo = half * h
        return lo, half, lo, lo + half // 2, half // 2, pos[h], pos[1 - h]

    def s1(r):
        if not 0 <= r < ROUNDS:
            return
        pack(r + 1)
        for h in range(2):
            lo, half, up, dn, quarter, p, q = geometry(r, h)
            own = block(r, h, p, q, lo, half)
            for d in range(2):
                send(own, own, y_send.at[r, h, d], y_recv.at[r, h, d], dev_axis[h][d])
            across(r, h, p)

    def across(r, h, p_at):
        lo, half, up, dn, quarter, p, q = geometry(r, h)
        piece = block(r, h, p_at, q, lo, half)
        for d in range(2):
            push(piece, piece, y_send.at[r, h, 4 + d], y_recv.at[r, h, 4 + d], dev_axis[1 - h][d])

    def s2(r):
        if not 0 <= r < ROUNDS:
            return
        for h in range(2):
            lo, half, up, dn, quarter, p, q = geometry(r, h)
            for d, at, part in ((0, (p + 3) % 4, up), (1, (p + 1) % 4, dn)):
                arrived(block(r, h, at, q, lo, half), y_recv.at[r, h, d])
                piece = block(r, h, at, q, part, quarter)
                send(piece, piece, y_send.at[r, h, 2 + d], y_recv.at[r, h, 2 + d], dev_axis[h][d])
                across(r, h, at)

    def s3(r):
        if not 0 <= r < ROUNDS:
            return
        for h in range(2):
            lo, half, up, dn, quarter, p, q = geometry(r, h)
            for d, part in ((0, up), (1, dn)):
                arrived(block(r, h, (p + 2) % 4, q, part, quarter), y_recv.at[r, h, 2 + d])
            across(r, h, (p + 2) % 4)
            for d in range(2):
                sent.append((line(r, h, q, lo, half), y_send.at[r, h, 4 + d]))

    def s4(r):
        if not 0 <= r < ROUNDS:
            return
        for h in range(2):
            lo, half, up, dn, quarter, p, q = geometry(r, h)
            for d, at, part in ((0, (q + 3) % 4, up), (1, (q + 1) % 4, dn)):
                arrived(line(r, h, at, lo, half), y_recv.at[r, h, 4 + d])
                for k in range(4):
                    piece = block(r, h, k, at, part, quarter)
                    push(piece, piece, y_send.at[r, h, 6 + d], y_recv.at[r, h, 6 + d], dev_axis[1 - h][d])
                sent.append((line(r, h, at, part, quarter), y_send.at[r, h, 6 + d]))

    def done(r):
        for h in range(2):
            lo, half, up, dn, quarter, p, q = geometry(r, h)
            for d, part in ((0, up), (1, dn)):
                arrived(line(r, h, (q + 2) % 4, part, quarter), y_recv.at[r, h, 6 + d])

    def ahead(k):
        s1(k + 2)
        s2(k + 1)
        s3(k)

    def tick(k):
        ahead(k)
        s4(k - 1)

    def gather_own(u, buf, s):
        src = buf.at[s, :, cols_of(1, core)]
        send(src, buf.at[s, :, cols_of(0, core)], a_send.at[u, 0], a_recv.at[u, 0], dev_xp)
        send(src, buf.at[s, :, cols_of(2, core)], a_send.at[u, 1], a_recv.at[u, 1], dev_xm)
        send(src, src, a_send.at[u, 2], a_recv.at[u, 4], dev_sib)

    def gather_near(u, buf, s):
        for d, place, lo, dev in ((0, 0, 0, dev_xp), (1, 2, HALF, dev_xm)):
            whole = buf.at[s, :, cols_of(place, core)]
            arrived(whole, a_recv.at[u, d])
            rows = pl.ds(lo, HALF)
            send(
                buf.at[s, rows, cols_of(place, core)], buf.at[s, rows, cols_of(3, core)],
                a_send.at[u, 3 + d], a_recv.at[u, 2 + d], dev,
            )
            send(whole, whole, a_send.at[u, 5 + d], a_recv.at[u, 5 + d], dev_sib)

    def gather_far(u, buf, s):
        for d, lo in ((0, 0), (1, HALF)):
            arrived(buf.at[s, pl.ds(lo, HALF), cols_of(3, core)], a_recv.at[u, 2 + d])
        whole = buf.at[s, :, cols_of(3, core)]
        send(whole, whole, a_send.at[u, 7], a_recv.at[u, 7], dev_sib)

    def near_done(u, buf, s):
        for k, place in ((4, 1), (5, 0), (6, 2)):
            arrived(buf.at[s, :, cols_of(place, 1 - core)], a_recv.at[u, k])

    def far_done(u, buf, s):
        arrived(buf.at[s, :, cols_of(3, 1 - core)], a_recv.at[u, 7])

    def add_squares(buf, s, places):
        total = None
        for j in range(4 * places[0], 4 * places[1]):
            v = buf[s, :, 128 * j : 128 * j + 128].astype(F32)
            total = v * v if total is None else total + v * v
        squares[s] = total if places[0] == 0 else squares[s] + total

    def row_factor(s):
        mean = jnp.sum(squares[s], axis=1, keepdims=True) * (1.0 / D)
        fac[s] = jnp.broadcast_to(lax.rsqrt(mean + EPS), (SEQ, 128))

    def shifted(v, n):
        turned = pltpu.roll(v, n, 0)
        row = lax.broadcasted_iota(jnp.int32, (8, v.shape[1]), 0)
        return jnp.concatenate([jnp.where(row >= n, turned[0:8], 0.0), turned[8:]], axis=0)

    def causal(v, taps):
        return shifted(v, 2) * taps[0:1] + shifted(v, 1) * taps[1:2] + v * taps[2:3]

    def wide(s):
        f = fac[s]
        return jnp.concatenate([f, f], axis=1)

    order = (3, 2, 0, 1)

    class Unit:
        def __init__(self, u, sems, sb, rb, keep, fbuf, nbuf, rf, rn):
            self.sb, self.rb, self.fbuf, self.nbuf, self.rf, self.rn = (
                ref.at[u] for ref in (sb, rb, fbuf, nbuf, rf, rn)
            )
            self.keep = keep
            self.ssem, self.rsem = r_send.at[sems], r_recv.at[sems]

        def part(self, k):
            send(self.sb.at[k], self.rb.at[k], self.ssem.at[k], self.rsem.at[k], dev_sib)

        def both(self, k, d):
            return self.keep(k, d) + self.rb[k, d].astype(F32)

        def far(self):
            arrived(self.rb.at[0], self.rsem.at[0])
            for d, dev in ((0, dev_xp), (1, dev_xm)):
                self.fbuf[d] = self.both(0, d).astype(BF)
            for d, dev in ((0, dev_xp), (1, dev_xm)):
                send(self.fbuf.at[d], self.rf.at[d], self.ssem.at[4 + d], self.rsem.at[4 + d], dev)

        def near(self):
            for d, dev in ((0, dev_xp), (1, dev_xm)):
                arrived(self.rb.at[1 + d], self.rsem.at[1 + d])
                self.nbuf[d, 1 - d] = self.both(1 + d, 1 - d).astype(BF)
            for d, dev in ((0, dev_xp), (1, dev_xm)):
                send(
                    self.nbuf.at[d, 1 - d], self.rn.at[d, 1 - d],
                    self.ssem.at[6 + d], self.rsem.at[6 + d], dev,
                )

        def last(self):
            for d, dev in ((0, dev_xp), (1, dev_xm)):
                arrived(self.rf.at[d], self.rsem.at[4 + d])
                self.nbuf[d, d] = (self.both(1 + d, d) + self.rf[d].astype(F32)).astype(BF)
                send(self.nbuf.at[d, d], self.rn.at[d, d], self.ssem.at[8 + d], self.rsem.at[8 + d], dev)

        def landed(self):
            arrived(self.rb.at[3], self.rsem.at[3])
            for d in range(2):
                arrived(self.rn.at[d, 1 - d], self.rsem.at[6 + d])
                arrived(self.rn.at[d, d], self.rsem.at[8 + d])

        def total(self, d):
            return self.both(3, d) + self.rn[0, d].astype(F32) + self.rn[1, d].astype(F32)

    def mix_unit(s):
        return Unit(s, s, sb, rb, lambda k, d: keep[s, k, d], fbuf, nbuf, rf, rn)

    def ffn_unit(h):
        return Unit(
            h, 2 + h, sb2, rb2, lambda k, d: keep2[h, order[k], 2 * core + d], fbuf2, nbuf2, rf2, rn2
        )

    def dot(a, b):
        return jnp.dot(a, b, preferred_element_type=F32)

    def in_cgate():
        @pl.loop(0, 2)
        def _(s):
            cbuf[s] = dot(tfull[s], g_in[0].reshape(D, W))

    def in_value():
        @pl.loop(0, 2)
        def _(s):
            f = wide(s)
            inner = dot(tfull[s], g_in[1].reshape(D, W)) * cbuf[s] * (f * f)
            cbuf[s] = causal(inner, mtaps) * f

    def in_bgate():
        @pl.loop(0, 2)
        def _(s):
            gated[s] = (dot(tfull[s], g_in[2].reshape(D, W)) * cbuf[s]).astype(BF)

    def mix_parts(s, unit):
        for cc in (1 - core, core):
            mat = jnp.concatenate([g_mo[0, place, 2 * cc + j] for place in order for j in range(2)], axis=1)
            term = dot(gated[s], mat)
            for k in range(4):
                piece = term[:, W * k : W * k + W].reshape(2, HALF, W)
                if cc is core:
                    keep[s, k] = piece
                else:
                    sb[s, k] = piece.astype(BF)
                    unit.part(k)

    def up_first(s, js):
        for j in js:
            if j < 5:
                acc[s, j] = dot(rfull[s, :, 0:1536], g_up[j, 0:3].reshape(1536, W))
            else:
                acc_tail[s] = dot(rfull[s, :, 0:1536], g_ul[0, 0:3].reshape(1536, 128))

    def tokens_of(s):
        return slice(SEQ * s, SEQ * s + SEQ)

    def silu(v):
        return v / (1.0 + jnp.exp(-v))

    def up_second(s):
        for j in range(5):
            cols = slice(128 * j, 128 * j + 128)
            pre = (acc[s, j] + dot(rfull[s, :, 1536:2048], g_up[j, 3].reshape(512, W))) * wide(s)
            taps = jnp.concatenate([ftaps[:, 0, cols], ftaps[:, 1, cols]], axis=1)
            conv = causal(pre, taps)
            active[cols, tokens_of(s)] = (silu(conv[:, 0:128]) * conv[:, 128:256]).T.astype(BF)
        pre = (acc_tail[s] + dot(rfull[s, :, 1536:2048], g_ul[0, 3].reshape(512, 128))) * fac[s]
        taps = jnp.concatenate([ftaps[:, 0, tail], ftaps[:, 1, tail]], axis=1)
        conv = causal(pre, taps)
        act = (silu(conv) * pltpu.roll(conv, 64, 1)).T[0:64].astype(BF)
        active[640:704, tokens_of(s)] = act
        active[832:896, tokens_of(s)] = act
        active[704:832, tokens_of(s)] = jnp.zeros((128, SEQ), BF)

    def down_parts(h, unit):
        lo = 640 + 128 * h
        acts = jnp.concatenate([active[0:640, :], active[lo : lo + 128, :]], axis=0)
        for first, ks in ((2, (0, 1)), (0, (2, 3))):
            places = slice(first, first + 2)
            mat = jnp.concatenate(
                [g_d[h, places].reshape(512, 640), g_dt[0, places].reshape(512, 128)], axis=1
            )
            keep2[h, places] = dot(mat, acts).reshape(2, 4, 64, 2 * SEQ)
            for k in ks:
                sb2[h, k] = keep2[h, order[k], pl.ds(2 * (1 - core), 2)].astype(BF)
                unit.part(k)

    own = cols_of(1, core)

    ready(("tok", 0), ("tok", 1))
    pl.semaphore_wait(barrier, 7)
    for s in range(2):
        gather_own(s, tfull, s)
    pack(0)
    s1(0)
    s1(1)
    s2(0)
    tick(0)
    gather_near(0, tfull, 0)
    tick(1)
    gather_near(1, tfull, 1)
    gather_far(0, tfull, 0)
    near_done(0, tfull, 0)
    add_squares(tfull, 0, (0, 3))
    tick(2)
    gather_far(1, tfull, 1)
    ready("mtaps", "ftaps")
    ahead(3)
    near_done(1, tfull, 1)
    add_squares(tfull, 1, (0, 3))
    for s in range(2):
        far_done(s, tfull, s)
        add_squares(tfull, s, (3, 4))
        row_factor(s)
    done(0)
    in_cgate()
    s4(2)
    ahead(4)
    done(1)
    in_value()
    s4(3)
    done(2)
    in_bgate()
    ahead(5)
    done(3)
    u0, u1 = mix_unit(0), mix_unit(1)
    mix_parts(0, u0)
    s4(4)
    s1(8)
    s2(7)
    u0.far()
    u0.near()
    s3(6)
    mix_parts(1, u1)
    s4(5)
    u1.far()
    u0.last()
    u1.near()
    s1(9)
    s2(8)
    s3(7)
    s4(6)
    s1(10)
    u1.last()
    s2(9)
    s1(11)
    s3(8)

    def residual(s, unit):
        unit.landed()
        for d in range(2):
            rows = slice(HALF * d, HALF * d + HALF)
            rfull[s, rows, own] = (tfull[s, rows, own].astype(F32) + unit.total(d)).astype(BF)
        gather_own(2 + s, rfull, s)

    residual(0, u0)
    s4(7)
    s2(10)
    residual(1, u1)
    s1(12)
    s3(9)
    s2(11)
    gather_near(2, rfull, 0)
    s4(8)
    s3(10)
    near_done(2, rfull, 0)
    add_squares(rfull, 0, (0, 3))
    for r in range(4, 8):
        done(r)
    s4(9)
    up_first(0, (0, 1, 2, 3))
    gather_near(3, rfull, 1)
    s2(12)
    s3(11)
    s4(10)
    done(8)
    done(9)
    up_first(0, (4, 5))
    near_done(3, rfull, 1)
    gather_far(2, rfull, 0)
    s3(12)
    s4(11)
    add_squares(rfull, 1, (0, 3))
    up_first(1, (0, 1, 2, 3, 4, 5))
    gather_far(3, rfull, 1)
    s4(12)
    for s in range(2):
        far_done(2 + s, rfull, s)
        add_squares(rfull, s, (3, 4))
        row_factor(s)
        up_second(s)
    done(10)
    done(11)
    v0, v1 = ffn_unit(0), ffn_unit(1)
    down_parts(0, v0)
    v0.far()
    v0.near()
    done(12)
    down_parts(1, v1)
    v1.far()
    v0.last()
    v1.near()
    v1.last()
    total = []
    for h, unit in enumerate((v0, v1)):
        unit.landed()
        total.append([unit.total(d) for d in range(2)])
    for s in range(2):
        for d in range(2):
            lanes = slice(SEQ * s, SEQ * s + SEQ)
            turned = jnp.concatenate([total[0][d][:, lanes], total[1][d][:, lanes]], axis=0).T
            cols = pl.ds(pl.multiple_of((2 + core) * W + 128 * d, 128), 128)
            out[s, :, 128 * d : 128 * d + 128] = (rfull[s, :, cols].astype(F32) + turned).astype(BF)
    for src, ssem in sent:
        arrived(src, ssem)


def on_device(
    tokens, mix_gain, w_bgate, w_cgate, w_value, in_scale, mix_taps, w_mixout, mixout_scale,
    ffn_gain, w_upgate, w_upval, up_scale, ffn_taps, w_down, down_scale,
):
    args = (
        tokens, mix_gain.reshape(16, 128), w_bgate, w_cgate, w_value, in_scale, mix_taps, w_mixout,
        mixout_scale, ffn_gain.reshape(16, 128), w_upgate.T, w_upval.T, up_scale,
        jnp.swapaxes(ffn_taps, 0, 1), w_down, down_scale,
    )
    vmem = pltpu.VMEM

    def exchange_buffers(piece, kept):
        return (
            vmem((2, 4, 2, *piece), BF),
            vmem((2, 4, 2, *piece), BF),
            vmem((2, 4, kept, *piece), F32),
            vmem((2, 2, *piece), BF),
            vmem((2, 2, 2, *piece), BF),
            vmem((2, 2, *piece), BF),
            vmem((2, 2, 2, *piece), BF),
        )

    dma = pltpu.SemaphoreType.DMA
    return pl.pallas_call(
        kernel,
        out_shape=jax.ShapeDtypeStruct(tokens.shape, BF),
        in_specs=[pl.BlockSpec(memory_space=pl.ANY)] * len(args),
        out_specs=pl.BlockSpec(memory_space=pltpu.VMEM),
        scratch_shapes=[
            *(vmem(a.shape, a.dtype) for a in args[1:]),
            vmem((3, 4, 4, 128, W), BF),
            vmem((1, 4, 4, 256, 128), BF),
            vmem((5, 4, 4, 128, W), BF),
            vmem((1, 4, 4, 128, 128), BF),
            vmem((1, 4, 4, 64, 128), BF),
            vmem((2, 4, 4, 64, 640), BF),
            vmem((2, SEQ, D), BF),
            vmem((2, SEQ, D), BF),
            vmem((2, SEQ, W), F32),
            vmem((2, SEQ, W), BF),
            vmem((896, 2 * SEQ), BF),
            vmem((2, SEQ, 128), F32),
            vmem((2, SEQ, 128), F32),
            vmem((2, 5, SEQ, W), F32),
            vmem((2, SEQ, 128), F32),
            *exchange_buffers((HALF, W), 2),
            *exchange_buffers((64, 2 * SEQ), 4),
            dma((ROUNDS, 2, 8)),
            dma((ROUNDS, 2, 8)),
            dma((4, 8)),
            dma((4, 8)),
            dma((4, 10)),
            dma((4, 10)),
            dma((17,)),
        ],
        compiler_params=pltpu.CompilerParams(
            collective_id=0, has_side_effects=True, vmem_limit_bytes=62 * 1024 * 1024
        ),
        name="layer",
    )(*args)


def solution(mesh):
    return jax.shard_map(
        on_device,
        mesh=mesh,
        in_specs=(
            P("fs", None, "tp"),
            P(),
            P("fs", "tp"),
            P("fs", "tp"),
            P("fs", "tp"),
            P(None, "tp"),
            P(None, "tp"),
            P("tp", "fs"),
            P(None, "fs"),
            P(),
            P("fs", "tp"),
            P("fs", "tp"),
            P(None, "tp"),
            P(None, None, "tp"),
            P("tp", "fs"),
            P(None, "fs"),
        ),
        out_specs=P("fs", None, "tp"),
        check_vma=False,
    )
```

```python
import functools

import jax
import jax.numpy as jnp
from jax import lax
from jax.experimental import pallas as pl
from jax.experimental.pallas import tpu as pltpu
from jax.sharding import PartitionSpec as P

EPS = 1e-06
BF = jnp.bfloat16
F32 = jnp.float32
SEQ = 384
HALF = SEQ // 2
D = 2048
W = 256
ROUNDS = 13


def kernel(
    tok_h, mgain_h, wb_h, wc_h, wv_h, insc_h, mtaps_h, wm_h, msc_h, fgain_h, wug_h, wuv_h, upsc_h, ftaps_h,
    wd_h, dsc_h,
    out,
    mgain, wb, wc, wv, insc, mtaps, wm, msc, fgain, wug, wuv, upsc, ftaps, wd, dsc,
    g_in, g_mo, g_up, g_ul, g_dt, g_d,
    tfull, rfull, cbuf, gated, active, fac, squares, acc, acc_tail,
    sb, rb, keep, fbuf, nbuf, rf, rn,
    sb2, rb2, keep2, fbuf2, nbuf2, rf2, rn2,
    y_send, y_recv, a_send, a_recv, r_send, r_recv, load_sem,
):
    fs = lax.axis_index("fs")
    tp = lax.axis_index("tp")
    z, y = fs // 4, fs % 4
    x, core = tp // 2, tp % 2
    xp, xm, xf = (x + 1) % 4, (x + 3) % 4, (x + 2) % 4
    dev_xp = (fs, xp * 2 + core)
    dev_xm = (fs, xm * 2 + core)
    dev_sib = (fs, x * 2 + 1 - core)
    dev_axis = (
        ((z * 4 + (y + 1) % 4, tp), (z * 4 + (y + 3) % 4, tp)),
        ((((z + 1) % 4) * 4 + y, tp), (((z + 3) % 4) * 4 + y, tp)),
    )
    pos = (y, z)
    sent = []

    def slot(zz):
        return (zz - x + 5) % 4


    def push(src, dst, ssem, rsem, dev):
        pltpu.make_async_remote_copy(
            src_ref=src, dst_ref=dst, send_sem=ssem, recv_sem=rsem,
            device_id=dev, device_id_type=pl.DeviceIdType.MESH,
        ).start()

    def arrived(dst, rsem):
        pltpu.make_async_copy(dst, dst, rsem).wait()

    barrier = pltpu.get_barrier_semaphore()
    for dev in (*dev_axis[0], *dev_axis[1], dev_xp, dev_xm, dev_sib):
        pl.semaphore_signal(barrier, inc=1, device_id=dev, device_id_type=pl.DeviceIdType.MESH)

    loads = {}

    def load(name, src, dst):
        loads[name] = pltpu.make_async_copy(src, dst, load_sem.at[len(loads)])
        loads[name].start()

    def cols_of(place, cc):
        return pl.ds(pl.multiple_of((place * 2 + cc) * W, W), W)

    load("tok", tok_h, tfull.at[:, :, cols_of(1, core)])
    for name, src, dst in (
        ("wc", wc_h, wc), ("mgain", mgain_h, mgain), ("insc", insc_h, insc), ("wv", wv_h, wv), ("wb", wb_h, wb),
        ("msc", msc_h, msc), ("wm", wm_h, wm), ("fgain", fgain_h, fgain), ("upsc", upsc_h, upsc),
        ("wug", wug_h, wug), ("wuv", wuv_h, wuv), ("dsc", dsc_h, dsc), ("wd", wd_h, wd),
        ("mtaps", mtaps_h, mtaps), ("ftaps", ftaps_h, ftaps),
    ):
        load(name, src, dst)

    def ready(*names):
        for name in names:
            if name in loads:
                loads.pop(name).wait()

    def rounded(w):
        return w.astype(BF).astype(F32)

    tail = slice(640, 704)

    mine = slot(z) * 4 + y

    def pack(r):
        if r < 3:
            w, row = ((wc, 1), (wv, 2), (wb, 0))[r]
            ready("mgain", "insc", ("wc", "wv", "wb")[r])
            col = jnp.broadcast_to(mgain[pl.ds(fs, 1), :], (128, 128)).T
            col = jnp.concatenate([col, col], axis=1)
            g_in[r, mine] = (rounded(w[...]) * col * insc[row : row + 1, :]).astype(BF)
        elif r == 3:
            ready("msc", "wm")
            g_mo[0, mine] = (rounded(wm[...]) * msc[...]).astype(BF)
        elif r < 9:
            ready("fgain", "upsc", "wug", "wuv")
            frow = fgain[pl.ds(fs, 1), :]
            j = r - 4
            cols = slice(128 * j, 128 * j + 128)
            for k, w in enumerate((wug, wuv)):
                g_up[j, mine, :, 128 * k : 128 * k + 128] = (
                    (rounded(w[cols, :]) * frow).T * upsc[k : k + 1, cols]
                ).astype(BF)
        elif r == 9:
            frow = fgain[pl.ds(fs, 1), :]
            both = rounded(jnp.concatenate([wug[tail, :], wuv[tail, :]], axis=0))
            tail_scale = jnp.concatenate([upsc[0:1, tail], upsc[1:2, tail]], axis=1)
            g_ul[0, mine] = ((both * frow).T * tail_scale).astype(BF)
        elif r == 10:
            ready("dsc", "wd")
            last = rounded(wd[tail, :]) * dsc[...]
            turned = jnp.concatenate([last, last], axis=0).T
            lane = lax.broadcasted_iota(jnp.int32, (64, 128), 1)
            g_dt[0, mine] = jnp.where(lane < 64, turned[0:64], turned[64:128]).astype(BF)
        elif r < 13:
            lo = 64 * (r - 11)
            for j in range(5):
                cols = slice(128 * j, 128 * j + 128)
                turned = (rounded(wd[cols, :]) * dsc[...]).T
                g_d[r - 11, mine, :, cols] = turned[lo : lo + 64].astype(BF)

    rounds = (
        [(g_in, k, 128) for k in range(3)]
        + [(g_mo, 0, 256)]
        + [(g_up, k, 128) for k in range(5)]
        + [(g_ul, 0, 128), (g_dt, 0, 64)]
        + [(g_d, k, 64) for k in range(2)]
    )

    def block(r, h, p_at, q_at, lo, n):
        ref, k, rows = rounds[r]
        zz, yy = (q_at, p_at) if h == 0 else (p_at, q_at)
        return ref.at[k, slot(zz) * 4 + yy, pl.ds(lo, n), :]

    def some(r, n, rows):
        ref, k, _ = rounds[r]
        return ref.at[k, pl.ds(0, n), pl.ds(0, rows), :]

    def geometry(r, h):
        half = rounds[r][2] // 2
        lo = half * h
        return lo, half, lo, lo + half // 2, half // 2, pos[h], pos[1 - h]

    def hop(r, h, stage, piece, axis, d):
        push(piece, piece, y_send.at[r], y_recv.at[r, 2 * stage + h if stage < 3 else 6], dev_axis[axis][d])

    def across(r, h, p_at):
        lo, half, up, dn, quarter, p, q = geometry(r, h)
        for d in range(2):
            hop(r, h, 2, block(r, h, p_at, q, lo, half), 1 - h, d)

    def s1(r):
        if not 0 <= r < ROUNDS:
            return
        pack(r + 1)
        for h in range(2):
            lo, half, up, dn, quarter, p, q = geometry(r, h)
            for d in range(2):
                hop(r, h, 0, block(r, h, p, q, lo, half), h, d)
            across(r, h, p)

    def s2(r):
        if not 0 <= r < ROUNDS:
            return
        for h in range(2):
            lo, half, up, dn, quarter, p, q = geometry(r, h)
            arrived(some(r, 2, half), y_recv.at[r, h])
            for d, at, part in ((0, (p + 3) % 4, up), (1, (p + 1) % 4, dn)):
                hop(r, h, 1, block(r, h, at, q, part, quarter), h, d)
            for at in ((p + 3) % 4, (p + 1) % 4):
                across(r, h, at)

    def s3(r):
        if not 0 <= r < ROUNDS:
            return
        for h in range(2):
            lo, half, up, dn, quarter, p, q = geometry(r, h)
            arrived(some(r, 2, quarter), y_recv.at[r, 2 + h])
            across(r, h, (p + 2) % 4)

    def s4(r):
        if not 0 <= r < ROUNDS:
            return
        for h in range(2):
            lo, half, up, dn, quarter, p, q = geometry(r, h)
            arrived(some(r, 8, half), y_recv.at[r, 4 + h])
            for d, at, part in ((0, (q + 3) % 4, up), (1, (q + 1) % 4, dn)):
                for k in range(4):
                    hop(r, h, 3, block(r, h, k, at, part, quarter), 1 - h, d)
        sent.append((some(r, 15, rounds[r][2]), y_send.at[r]))

    def done(r):
        arrived(some(r, 16, rounds[r][2] // 4), y_recv.at[r, 6])

    def ahead(k):
        s1(k + 2)
        s2(k + 1)
        s3(k)

    def tick(k):
        ahead(k)
        s4(k - 1)

    def gather_own(u, buf, s):
        src = buf.at[s, :, cols_of(1, core)]
        push(src, buf.at[s, :, cols_of(0, core)], a_send.at[u], a_recv.at[u, 0], dev_xp)
        push(src, buf.at[s, :, cols_of(2, core)], a_send.at[u], a_recv.at[u, 1], dev_xm)
        push(src, src, a_send.at[u], a_recv.at[u, 3], dev_sib)

    def gather_near(u, buf, s):
        for d, place, lo, dev in ((0, 0, 0, dev_xp), (1, 2, HALF, dev_xm)):
            whole = buf.at[s, :, cols_of(place, core)]
            arrived(whole, a_recv.at[u, d])
            rows = pl.ds(lo, HALF)
            push(
                buf.at[s, rows, cols_of(place, core)], buf.at[s, rows, cols_of(3, core)],
                a_send.at[u], a_recv.at[u, 2], dev,
            )
            push(whole, whole, a_send.at[u], a_recv.at[u, 3], dev_sib)

    def gather_far(u, buf, s):
        whole = buf.at[s, :, cols_of(3, core)]
        arrived(whole, a_recv.at[u, 2])
        push(whole, whole, a_send.at[u], a_recv.at[u, 4], dev_sib)
        sent.append((sb.at[pl.ds(0, 14)], a_send.at[u]))

    def near_done(u, buf, s):
        arrived(buf.at[s, :, pl.ds(0, 3 * W)], a_recv.at[u, 3])

    def far_done(u, buf, s):
        arrived(buf.at[s, :, cols_of(3, 1 - core)], a_recv.at[u, 4])

    def add_squares(buf, s, places):
        total = None
        for j in range(4 * places[0], 4 * places[1]):
            v = buf[s, :, 128 * j : 128 * j + 128].astype(F32)
            total = v * v if total is None else total + v * v
        squares[s] = total if places[0] == 0 else squares[s] + total

    def row_factor(s):
        mean = jnp.sum(squares[s], axis=1, keepdims=True) * (1.0 / D)
        fac[s] = jnp.broadcast_to(lax.rsqrt(mean + EPS), (SEQ, 128))

    def shifted(v, n):
        turned = pltpu.roll(v, n, 0)
        row = lax.broadcasted_iota(jnp.int32, (8, v.shape[1]), 0)
        return jnp.concatenate([jnp.where(row >= n, turned[0:8], 0.0), turned[8:]], axis=0)

    def causal(v, taps):
        return shifted(v, 2) * taps[0:1] + shifted(v, 1) * taps[1:2] + v * taps[2:3]

    def wide(s):
        f = fac[s]
        return jnp.concatenate([f, f], axis=1)

    order = (3, 2, 0, 1)

    class Unit:
        def __init__(self, u, sems, sb, rb, keep, fbuf, nbuf, rf, rn):
            self.fbuf, self.nbuf, self.rf, self.rn = (ref.at[u] for ref in (fbuf, nbuf, rf, rn))
            self.sb, self.rb, self.base = sb, rb, 8 * u
            self.keep = keep
            self.ssem, self.rsem = r_send.at[sems], r_recv.at[sems]

        def pieces(self, ref, k, n=1):
            return ref.at[pl.ds(self.base + 2 * k, 2 * n)]

        def part(self, k):
            push(
                self.pieces(self.sb, k), self.pieces(self.rb, k),
                self.ssem, self.rsem.at[(0, 1, 1, 3)[k]], dev_sib,
            )

        def both(self, k, d):
            return self.keep(k, d) + self.rb[self.base + 2 * k + d].astype(F32)

        def far(self):
            arrived(self.pieces(self.rb, 0), self.rsem.at[0])
            for d in range(2):
                self.fbuf[d] = self.both(0, d).astype(BF)
            for d, dev in ((0, dev_xp), (1, dev_xm)):
                push(self.fbuf.at[d], self.rf.at[d], self.ssem, self.rsem.at[2], dev)

        def near(self):
            arrived(self.pieces(self.rb, 1, 2), self.rsem.at[1])
            for d in range(2):
                self.nbuf[d, 1 - d] = self.both(1 + d, 1 - d).astype(BF)
            for d, dev in ((0, dev_xp), (1, dev_xm)):
                push(self.nbuf.at[d, 1 - d], self.rn.at[d, 1 - d], self.ssem, self.rsem.at[3], dev)

        def last(self):
            arrived(self.rf, self.rsem.at[2])
            for d in range(2):
                self.nbuf[d, d] = (self.both(1 + d, d) + self.rf[d].astype(F32)).astype(BF)
            for d, dev in ((0, dev_xp), (1, dev_xm)):
                push(self.nbuf.at[d, d], self.rn.at[d, d], self.ssem, self.rsem.at[3], dev)
            sent.append((sb.at[pl.ds(0, 14)], self.ssem))

        def landed(self):
            arrived(self.rb.at[pl.ds(0, 6)], self.rsem.at[3])

        def total(self, d):
            return self.both(3, d) + self.rn[0, d].astype(F32) + self.rn[1, d].astype(F32)

    def mix_unit(s):
        return Unit(s, s, sb, rb, lambda k, d: keep[s, k, d], fbuf, nbuf, rf, rn)

    def ffn_unit(h):
        return Unit(
            h, 2 + h, sb2, rb2, lambda k, d: keep2[h, 4 * order[k] + 2 * core + d], fbuf2, nbuf2, rf2, rn2
        )

    def dot(a, b):
        return jnp.dot(a, b, preferred_element_type=F32)

    def in_cgate():
        @pl.loop(0, 2)
        def _(s):
            cbuf[s] = dot(tfull[s], g_in[0].reshape(D, W))

    def in_value():
        @pl.loop(0, 2)
        def _(s):
            f = wide(s)
            inner = dot(tfull[s], g_in[1].reshape(D, W)) * cbuf[s] * (f * f)
            cbuf[s] = causal(inner, mtaps) * f

    def in_bgate():
        @pl.loop(0, 2)
        def _(s):
            gated[s] = (dot(tfull[s], g_in[2].reshape(D, W)) * cbuf[s]).astype(BF)

    def mix_parts(s, unit):
        for cc in (1 - core, core):
            mat = jnp.concatenate([g_mo[0, 4 * place + 2 * cc + j] for place in order for j in range(2)], axis=1)
            term = dot(gated[s], mat)
            for k in range(4):
                piece = term[:, W * k : W * k + W].reshape(2, HALF, W)
                if cc is core:
                    keep[s, k] = piece
                else:
                    sb[8 * s + 2 * k : 8 * s + 2 * k + 2] = piece.astype(BF)
                    unit.part(k)

    def up_first(s, js):
        for j in js:
            if j < 5:
                acc[s, j] = dot(rfull[s, :, 0:1536], g_up[j, 0:12].reshape(1536, W))
            else:
                acc_tail[s] = dot(rfull[s, :, 0:1536], g_ul[0, 0:12].reshape(1536, 128))

    def tokens_of(s):
        return slice(SEQ * s, SEQ * s + SEQ)

    def silu(v):
        return v / (1.0 + jnp.exp(-v))

    def up_second(s):
        for j in range(5):
            cols = slice(128 * j, 128 * j + 128)
            pre = (acc[s, j] + dot(rfull[s, :, 1536:2048], g_up[j, 12:16].reshape(512, W))) * wide(s)
            taps = jnp.concatenate([ftaps[:, 0, cols], ftaps[:, 1, cols]], axis=1)
            conv = causal(pre, taps)
            active[cols, tokens_of(s)] = (silu(conv[:, 0:128]) * conv[:, 128:256]).T.astype(BF)
        pre = (acc_tail[s] + dot(rfull[s, :, 1536:2048], g_ul[0, 12:16].reshape(512, 128))) * fac[s]
        taps = jnp.concatenate([ftaps[:, 0, tail], ftaps[:, 1, tail]], axis=1)
        conv = causal(pre, taps)
        act = (silu(conv) * pltpu.roll(conv, 64, 1)).T[0:64].astype(BF)
        active[640:704, tokens_of(s)] = act
        active[832:896, tokens_of(s)] = act
        active[704:832, tokens_of(s)] = jnp.zeros((128, SEQ), BF)

    def down_parts(h, unit):
        lo = 640 + 128 * h
        acts = jnp.concatenate([active[0:640, :], active[lo : lo + 128, :]], axis=0)
        for first, ks in ((2, (0, 1)), (0, (2, 3))):
            places = slice(4 * first, 4 * first + 8)
            mat = jnp.concatenate(
                [g_d[h, places].reshape(512, 640), g_dt[0, places].reshape(512, 128)], axis=1
            )
            keep2[h, places] = dot(mat, acts).reshape(8, 64, 2 * SEQ)
            for k in ks:
                piece = keep2[h, pl.ds(4 * order[k] + 2 * (1 - core), 2)].astype(BF)
                sb2[8 * h + 2 * k : 8 * h + 2 * k + 2] = piece
                unit.part(k)

    own = cols_of(1, core)

    pack(0)
    ready("tok")
    pl.semaphore_wait(barrier, 7)
    s1(0)
    for s in range(2):
        gather_own(s, tfull, s)
    s1(1)
    s1(2)
    s2(0)
    s2(1)
    s3(0)
    gather_near(0, tfull, 0)
    tick(1)
    gather_near(1, tfull, 1)
    gather_far(0, tfull, 0)
    near_done(0, tfull, 0)
    add_squares(tfull, 0, (0, 3))
    tick(2)
    gather_far(1, tfull, 1)
    ready("mtaps", "ftaps")
    ahead(3)
    near_done(1, tfull, 1)
    add_squares(tfull, 1, (0, 3))
    for s in range(2):
        far_done(s, tfull, s)
        add_squares(tfull, s, (3, 4))
        row_factor(s)
    done(0)
    in_cgate()
    s4(2)
    ahead(4)
    done(1)
    in_value()
    s4(3)
    done(2)
    in_bgate()
    ahead(5)
    done(3)
    u0, u1 = mix_unit(0), mix_unit(1)
    mix_parts(0, u0)
    s4(4)
    s1(8)
    s2(7)
    u0.far()
    u0.near()
    s3(6)
    mix_parts(1, u1)
    s4(5)
    u1.far()
    u0.last()
    u1.near()
    s1(9)
    s2(8)
    s3(7)
    s4(6)
    s1(10)
    u1.last()
    s2(9)
    s1(11)
    s3(8)

    def residual(s, unit):
        unit.landed()
        for d in range(2):
            rows = slice(HALF * d, HALF * d + HALF)
            rfull[s, rows, own] = (tfull[s, rows, own].astype(F32) + unit.total(d)).astype(BF)
        gather_own(2 + s, rfull, s)

    residual(0, u0)
    s4(7)
    s2(10)
    residual(1, u1)
    s1(12)
    s3(9)
    s2(11)
    gather_near(2, rfull, 0)
    s4(8)
    s3(10)
    near_done(2, rfull, 0)
    add_squares(rfull, 0, (0, 3))
    for r in range(4, 8):
        done(r)
    s4(9)
    up_first(0, (0, 1, 2, 3))
    gather_near(3, rfull, 1)
    s2(12)
    s3(11)
    s4(10)
    gather_far(2, rfull, 0)
    done(8)
    done(9)
    up_first(0, (4, 5))
    near_done(3, rfull, 1)
    add_squares(rfull, 1, (0, 3))
    up_first(1, (0, 1, 2, 3, 4, 5))
    s3(12)
    gather_far(3, rfull, 1)

    def finish(s):
        far_done(2 + s, rfull, s)
        add_squares(rfull, s, (3, 4))
        row_factor(s)
        up_second(s)

    finish(0)
    s4(11)
    finish(1)
    s4(12)
    done(10)
    done(11)
    v0, v1 = ffn_unit(0), ffn_unit(1)
    down_parts(0, v0)
    v0.far()
    v0.near()
    done(12)
    down_parts(1, v1)
    v1.far()
    v0.last()
    v1.near()
    v1.last()
    for src, ssem in sent:
        arrived(src, ssem)
    total = []
    for h, unit in enumerate((v0, v1)):
        unit.landed()
        total.append([unit.total(d) for d in range(2)])
    for s in range(2):
        for d in range(2):
            lanes = slice(SEQ * s, SEQ * s + SEQ)
            turned = jnp.concatenate([total[0][d][:, lanes], total[1][d][:, lanes]], axis=0).T
            cols = pl.ds(pl.multiple_of((2 + core) * W + 128 * d, 128), 128)
            out[s, :, 128 * d : 128 * d + 128] = (rfull[s, :, cols].astype(F32) + turned).astype(BF)


def on_device(
    tokens, mix_gain, w_bgate, w_cgate, w_value, in_scale, mix_taps, w_mixout, mixout_scale,
    ffn_gain, w_upgate, w_upval, up_scale, ffn_taps, w_down, down_scale,
):
    args = (
        tokens, mix_gain.reshape(16, 128), w_bgate, w_cgate, w_value, in_scale, mix_taps, w_mixout,
        mixout_scale, ffn_gain.reshape(16, 128), w_upgate.T, w_upval.T, up_scale,
        jnp.swapaxes(ffn_taps, 0, 1), w_down, down_scale,
    )
    vmem = pltpu.VMEM

    def exchange_buffers(piece, kept):
        return (
            vmem((16, *piece), BF),
            vmem((16, *piece), BF),
            vmem((2, *kept, *piece), F32),
            vmem((2, 2, *piece), BF),
            vmem((2, 2, 2, *piece), BF),
            vmem((2, 2, *piece), BF),
            vmem((2, 2, 2, *piece), BF),
        )

    dma = pltpu.SemaphoreType.DMA
    return pl.pallas_call(
        kernel,
        out_shape=jax.ShapeDtypeStruct(tokens.shape, BF),
        in_specs=[pl.BlockSpec(memory_space=pl.ANY)] * len(args),
        out_specs=pl.BlockSpec(memory_space=pltpu.VMEM),
        scratch_shapes=[
            *(vmem(a.shape, a.dtype) for a in args[1:]),
            vmem((3, 16, 128, W), BF),
            vmem((1, 16, 256, 128), BF),
            vmem((5, 16, 128, W), BF),
            vmem((1, 16, 128, 128), BF),
            vmem((1, 16, 64, 128), BF),
            vmem((2, 16, 64, 640), BF),
            vmem((2, SEQ, D), BF),
            vmem((2, SEQ, D), BF),
            vmem((2, SEQ, W), F32),
            vmem((2, SEQ, W), BF),
            vmem((896, 2 * SEQ), BF),
            vmem((2, SEQ, 128), F32),
            vmem((2, SEQ, 128), F32),
            vmem((2, 5, SEQ, W), F32),
            vmem((2, SEQ, 128), F32),
            *exchange_buffers((HALF, W), (4, 2)),
            *exchange_buffers((64, 2 * SEQ), (16,)),
            dma((ROUNDS,)),
            dma((ROUNDS, 7)),
            dma((4,)),
            dma((4, 5)),
            dma((4,)),
            dma((4, 4)),
            dma((16,)),
        ],
        compiler_params=pltpu.CompilerParams(
            collective_id=0, has_side_effects=True, vmem_limit_bytes=62 * 1024 * 1024
        ),
        name="layer",
    )(*args)


def solution(mesh):
    return jax.shard_map(
        on_device,
        mesh=mesh,
        in_specs=(
            P("fs", None, "tp"),
            P(),
            P("fs", "tp"),
            P("fs", "tp"),
            P("fs", "tp"),
            P(None, "tp"),
            P(None, "tp"),
            P("tp", "fs"),
            P(None, "fs"),
            P(),
            P("fs", "tp"),
            P("fs", "tp"),
            P(None, "tp"),
            P(None, None, "tp"),
            P("tp", "fs"),
            P(None, "fs"),
        ),
        out_specs=P("fs", None, "tp"),
        check_vma=False,
    )
```

```python
import functools

import jax
import jax.numpy as jnp
from jax import lax
from jax.experimental import pallas as pl
from jax.experimental.pallas import tpu as pltpu
from jax.sharding import PartitionSpec as P

EPS = 1e-06
BF = jnp.bfloat16
F32 = jnp.float32
SEQ = 384
HALF = SEQ // 2
D = 2048
W = 256
ROUNDS = 13


def kernel(
    tok_h, mgain_h, wb_h, wc_h, wv_h, insc_h, mtaps_h, wm_h, msc_h, fgain_h, wug_h, wuv_h, upsc_h, ftaps_h,
    wd_h, dsc_h,
    out,
    mgain, wb, wc, wv, insc, mtaps, wm, msc, fgain, wug, wuv, upsc, ftaps, wd, dsc,
    g_in, g_mo, g_up, g_ul, g_dt, g_d,
    tfull, rfull, cbuf, gated, active, fac, squares, acc, acc_tail,
    sb, rb, keep, fbuf, nbuf, rf, rn,
    sb2, rb2, keep2, fbuf2, nbuf2, rf2, rn2,
    y_send, y_recv, a_send, a_recv, r_send, r_recv, load_sem,
):
    fs = lax.axis_index("fs")
    tp = lax.axis_index("tp")
    z, y = fs // 4, fs % 4
    x, core = tp // 2, tp % 2
    xp, xm, xf = (x + 1) % 4, (x + 3) % 4, (x + 2) % 4
    dev_xp = (fs, xp * 2 + core)
    dev_xm = (fs, xm * 2 + core)
    dev_sib = (fs, x * 2 + 1 - core)
    dev_axis = (
        ((z * 4 + (y + 1) % 4, tp), (z * 4 + (y + 3) % 4, tp)),
        ((((z + 1) % 4) * 4 + y, tp), (((z + 3) % 4) * 4 + y, tp)),
    )
    pos = (y, z)
    sent = []

    def slot(zz):
        return (zz - x + 5) % 4


    def push(src, dst, ssem, rsem, dev):
        pltpu.make_async_remote_copy(
            src_ref=src, dst_ref=dst, send_sem=ssem, recv_sem=rsem,
            device_id=dev, device_id_type=pl.DeviceIdType.MESH,
        ).start()

    def arrived(dst, rsem):
        pltpu.make_async_copy(dst, dst, rsem).wait()

    barrier = pltpu.get_barrier_semaphore()
    for dev in (*dev_axis[0], *dev_axis[1], dev_xp, dev_xm, dev_sib):
        pl.semaphore_signal(barrier, inc=1, device_id=dev, device_id_type=pl.DeviceIdType.MESH)

    loads = {}

    def load(name, src, dst):
        loads[name] = pltpu.make_async_copy(src, dst, load_sem.at[len(loads)])
        loads[name].start()

    def cols_of(place, cc):
        return pl.ds(pl.multiple_of((place * 2 + cc) * W, W), W)

    load("tok", tok_h, tfull.at[:, :, cols_of(1, core)])
    for name, src, dst in (
        ("wc", wc_h, wc), ("mgain", mgain_h, mgain), ("insc", insc_h, insc), ("wv", wv_h, wv), ("wb", wb_h, wb),
        ("msc", msc_h, msc), ("wm", wm_h, wm), ("fgain", fgain_h, fgain), ("upsc", upsc_h, upsc),
        ("wug", wug_h, wug), ("wuv", wuv_h, wuv), ("dsc", dsc_h, dsc), ("wd", wd_h, wd),
        ("mtaps", mtaps_h, mtaps), ("ftaps", ftaps_h, ftaps),
    ):
        load(name, src, dst)

    def ready(*names):
        for name in names:
            if name in loads:
                loads.pop(name).wait()

    def rounded(w):
        return w.astype(BF).astype(F32)

    tail = slice(640, 704)

    mine = slot(z) * 4 + y

    def pack(r):
        if r < 3:
            w, row = ((wc, 1), (wv, 2), (wb, 0))[r]
            ready("mgain", "insc", ("wc", "wv", "wb")[r])
            col = jnp.broadcast_to(mgain[pl.ds(fs, 1), :], (128, 128)).T
            col = jnp.concatenate([col, col], axis=1)
            g_in[r, mine] = (rounded(w[...]) * col * insc[row : row + 1, :]).astype(BF)
        elif r == 3:
            ready("msc", "wm")
            g_mo[0, mine] = (rounded(wm[...]) * msc[...]).astype(BF)
        elif r < 9:
            ready("fgain", "upsc", "wug", "wuv")
            frow = fgain[pl.ds(fs, 1), :]
            j = r - 4
            cols = slice(128 * j, 128 * j + 128)
            for k, w in enumerate((wug, wuv)):
                g_up[j, mine, :, 128 * k : 128 * k + 128] = (
                    (rounded(w[cols, :]) * frow).T * upsc[k : k + 1, cols]
                ).astype(BF)
        elif r == 9:
            frow = fgain[pl.ds(fs, 1), :]
            both = rounded(jnp.concatenate([wug[tail, :], wuv[tail, :]], axis=0))
            tail_scale = jnp.concatenate([upsc[0:1, tail], upsc[1:2, tail]], axis=1)
            g_ul[0, mine] = ((both * frow).T * tail_scale).astype(BF)
        elif r == 10:
            ready("dsc", "wd")
            last = rounded(wd[tail, :]) * dsc[...]
            turned = jnp.concatenate([last, last], axis=0).T
            lane = lax.broadcasted_iota(jnp.int32, (64, 128), 1)
            g_dt[0, mine] = jnp.where(lane < 64, turned[0:64], turned[64:128]).astype(BF)
        elif r < 13:
            lo = 64 * (r - 11)
            for j in range(5):
                cols = slice(128 * j, 128 * j + 128)
                turned = (rounded(wd[cols, :]) * dsc[...]).T
                g_d[r - 11, mine, :, cols] = turned[lo : lo + 64].astype(BF)

    rounds = (
        [(g_in, k, 128) for k in range(3)]
        + [(g_mo, 0, 256)]
        + [(g_up, k, 128) for k in range(5)]
        + [(g_ul, 0, 128), (g_dt, 0, 64)]
        + [(g_d, k, 64) for k in range(2)]
    )

    def block(r, h, p_at, q_at, lo, n):
        ref, k, rows = rounds[r]
        zz, yy = (q_at, p_at) if h == 0 else (p_at, q_at)
        return ref.at[k, slot(zz) * 4 + yy, pl.ds(lo, n), :]

    def some(r, n, rows):
        ref, k, _ = rounds[r]
        return ref.at[k, pl.ds(0, n), pl.ds(0, rows), :]

    def geometry(r, h):
        half = rounds[r][2] // 2
        lo = half * h
        return lo, half, lo, lo + half // 2, half // 2, pos[h], pos[1 - h]

    def hop(r, h, stage, piece, axis, d):
        push(piece, piece, y_send.at[r], y_recv.at[r, 2 * stage + h if stage < 3 else 6], dev_axis[axis][d])

    def across(r, h, p_at):
        lo, half, up, dn, quarter, p, q = geometry(r, h)
        for d in range(2):
            hop(r, h, 2, block(r, h, p_at, q, lo, half), 1 - h, d)

    def s1(r):
        if not 0 <= r < ROUNDS:
            return
        pack(r + 1)
        for h in range(2):
            lo, half, up, dn, quarter, p, q = geometry(r, h)
            for d in range(2):
                hop(r, h, 0, block(r, h, p, q, lo, half), h, d)
            across(r, h, p)

    def s2(r):
        if not 0 <= r < ROUNDS:
            return
        for h in range(2):
            lo, half, up, dn, quarter, p, q = geometry(r, h)
            arrived(some(r, 2, half), y_recv.at[r, h])
            for d, at, part in ((0, (p + 3) % 4, up), (1, (p + 1) % 4, dn)):
                hop(r, h, 1, block(r, h, at, q, part, quarter), h, d)
            for at in ((p + 3) % 4, (p + 1) % 4):
                across(r, h, at)

    def s3(r):
        if not 0 <= r < ROUNDS:
            return
        for h in range(2):
            lo, half, up, dn, quarter, p, q = geometry(r, h)
            arrived(some(r, 2, quarter), y_recv.at[r, 2 + h])
            across(r, h, (p + 2) % 4)

    def s4(r):
        if not 0 <= r < ROUNDS:
            return
        for h in range(2):
            lo, half, up, dn, quarter, p, q = geometry(r, h)
            arrived(some(r, 8, half), y_recv.at[r, 4 + h])
            for d, at, part in ((0, (q + 3) % 4, up), (1, (q + 1) % 4, dn)):
                for k in range(4):
                    hop(r, h, 3, block(r, h, k, at, part, quarter), 1 - h, d)
        sent.append((some(r, 15, rounds[r][2]), y_send.at[r]))

    def done(r):
        arrived(some(r, 16, rounds[r][2] // 4), y_recv.at[r, 6])

    def ahead(k):
        s1(k + 2)
        s2(k + 1)
        s3(k)

    def tick(k):
        ahead(k)
        s4(k - 1)

    def gather_own(u, buf, s):
        src = buf.at[s, :, cols_of(1, core)]
        push(src, buf.at[s, :, cols_of(0, core)], a_send.at[u], a_recv.at[u, 0], dev_xp)
        push(src, buf.at[s, :, cols_of(2, core)], a_send.at[u], a_recv.at[u, 1], dev_xm)
        push(src, src, a_send.at[u], a_recv.at[u, 3], dev_sib)

    def gather_near(u, buf, s):
        for d, place, lo, dev in ((0, 0, 0, dev_xp), (1, 2, HALF, dev_xm)):
            whole = buf.at[s, :, cols_of(place, core)]
            arrived(whole, a_recv.at[u, d])
            rows = pl.ds(lo, HALF)
            push(
                buf.at[s, rows, cols_of(place, core)], buf.at[s, rows, cols_of(3, core)],
                a_send.at[u], a_recv.at[u, 2], dev,
            )
            push(whole, whole, a_send.at[u], a_recv.at[u, 3], dev_sib)

    def gather_far(u, buf, s):
        whole = buf.at[s, :, cols_of(3, core)]
        arrived(whole, a_recv.at[u, 2])
        push(whole, whole, a_send.at[u], a_recv.at[u, 4], dev_sib)
        sent.append((sb.at[pl.ds(0, 14)], a_send.at[u]))

    def near_done(u, buf, s):
        arrived(buf.at[s, :, pl.ds(0, 3 * W)], a_recv.at[u, 3])

    def far_done(u, buf, s):
        arrived(buf.at[s, :, cols_of(3, 1 - core)], a_recv.at[u, 4])

    def add_squares(buf, s, places):
        total = None
        for j in range(4 * places[0], 4 * places[1]):
            v = buf[s, :, 128 * j : 128 * j + 128].astype(F32)
            total = v * v if total is None else total + v * v
        squares[s] = total if places[0] == 0 else squares[s] + total

    def row_factor(s):
        mean = jnp.sum(squares[s], axis=1, keepdims=True) * (1.0 / D)
        fac[s] = jnp.broadcast_to(lax.rsqrt(mean + EPS), (SEQ, 128))

    def shifted(v, n):
        turned = pltpu.roll(v, n, 0)
        row = lax.broadcasted_iota(jnp.int32, (8, v.shape[1]), 0)
        return jnp.concatenate([jnp.where(row >= n, turned[0:8], 0.0), turned[8:]], axis=0)

    def causal(v, taps):
        return shifted(v, 2) * taps[0:1] + shifted(v, 1) * taps[1:2] + v * taps[2:3]

    def wide(s):
        f = fac[s]
        return jnp.concatenate([f, f], axis=1)

    order = (3, 2, 0, 1)

    class Unit:
        def __init__(self, u, sems, sb, rb, keep, fbuf, nbuf, rf, rn):
            self.fbuf, self.nbuf, self.rf, self.rn = (ref.at[u] for ref in (fbuf, nbuf, rf, rn))
            self.sb, self.rb, self.base = sb, rb, 8 * u
            self.keep = keep
            self.ssem, self.rsem = r_send.at[sems], r_recv.at[sems]

        def pieces(self, ref, k, n=1):
            return ref.at[pl.ds(self.base + 2 * k, 2 * n)]

        def part(self, k):
            push(
                self.pieces(self.sb, k), self.pieces(self.rb, k),
                self.ssem, self.rsem.at[(0, 1, 1, 3)[k]], dev_sib,
            )

        def both(self, k, d):
            return self.keep(k, d) + self.rb[self.base + 2 * k + d].astype(F32)

        def far(self):
            arrived(self.pieces(self.rb, 0), self.rsem.at[0])
            for d in range(2):
                self.fbuf[d] = self.both(0, d).astype(BF)
            for d, dev in ((0, dev_xp), (1, dev_xm)):
                push(self.fbuf.at[d], self.rf.at[d], self.ssem, self.rsem.at[2], dev)

        def near(self):
            arrived(self.pieces(self.rb, 1, 2), self.rsem.at[1])
            for d in range(2):
                self.nbuf[d, 1 - d] = self.both(1 + d, 1 - d).astype(BF)
            for d, dev in ((0, dev_xp), (1, dev_xm)):
                push(self.nbuf.at[d, 1 - d], self.rn.at[d, 1 - d], self.ssem, self.rsem.at[3], dev)

        def last(self):
            arrived(self.rf, self.rsem.at[2])
            for d in range(2):
                self.nbuf[d, d] = (self.both(1 + d, d) + self.rf[d].astype(F32)).astype(BF)
            for d, dev in ((0, dev_xp), (1, dev_xm)):
                push(self.nbuf.at[d, d], self.rn.at[d, d], self.ssem, self.rsem.at[3], dev)
            sent.append((sb.at[pl.ds(0, 14)], self.ssem))

        def landed(self):
            arrived(self.rb.at[pl.ds(0, 6)], self.rsem.at[3])

        def total(self, d):
            return self.both(3, d) + self.rn[0, d].astype(F32) + self.rn[1, d].astype(F32)

    def mix_unit(s):
        return Unit(s, s, sb, rb, lambda k, d: keep[s, k, d], fbuf, nbuf, rf, rn)

    def ffn_unit(h):
        return Unit(
            h, 2 + h, sb2, rb2, lambda k, d: keep2[h, 2 * k + d], fbuf2, nbuf2, rf2, rn2
        )

    def dot(a, b):
        return jnp.dot(a, b, preferred_element_type=F32)

    def in_cgate():
        @pl.loop(0, 2)
        def _(s):
            cbuf[s] = dot(tfull[s], g_in[0].reshape(D, W))

    def in_value():
        @pl.loop(0, 2)
        def _(s):
            f = wide(s)
            inner = dot(tfull[s], g_in[1].reshape(D, W)) * cbuf[s] * (f * f)
            cbuf[s] = causal(inner, mtaps) * f

    def in_bgate():
        @pl.loop(0, 2)
        def _(s):
            gated[s] = (dot(tfull[s], g_in[2].reshape(D, W)) * cbuf[s]).astype(BF)

    def mix_parts(s, unit):
        for cc in (1 - core, core):
            mat = jnp.concatenate([g_mo[0, 4 * place + 2 * cc + j] for place in order for j in range(2)], axis=1)
            term = dot(gated[s], mat)
            for k in range(4):
                piece = term[:, W * k : W * k + W].reshape(2, HALF, W)
                if cc is core:
                    keep[s, k] = piece
                else:
                    sb[8 * s + 2 * k : 8 * s + 2 * k + 2] = piece.astype(BF)
                    unit.part(k)

    def up_first(s, js):
        for j in js:
            if j < 5:
                acc[s, j] = dot(rfull[s, :, 0:1536], g_up[j, 0:12].reshape(1536, W))
            else:
                acc_tail[s] = dot(rfull[s, :, 0:1536], g_ul[0, 0:12].reshape(1536, 128))

    def tokens_of(s):
        return slice(SEQ * s, SEQ * s + SEQ)

    def silu(v):
        return v / (1.0 + jnp.exp(-v))

    def up_second(s):
        for j in range(5):
            cols = slice(128 * j, 128 * j + 128)
            pre = (acc[s, j] + dot(rfull[s, :, 1536:2048], g_up[j, 12:16].reshape(512, W))) * wide(s)
            taps = jnp.concatenate([ftaps[:, 0, cols], ftaps[:, 1, cols]], axis=1)
            conv = causal(pre, taps)
            active[cols, tokens_of(s)] = (silu(conv[:, 0:128]) * conv[:, 128:256]).T.astype(BF)
        pre = (acc_tail[s] + dot(rfull[s, :, 1536:2048], g_ul[0, 12:16].reshape(512, 128))) * fac[s]
        taps = jnp.concatenate([ftaps[:, 0, tail], ftaps[:, 1, tail]], axis=1)
        conv = causal(pre, taps)
        act = (silu(conv) * pltpu.roll(conv, 64, 1)).T[0:64].astype(BF)
        active[640:704, tokens_of(s)] = act
        active[832:896, tokens_of(s)] = act
        active[704:832, tokens_of(s)] = jnp.zeros((128, SEQ), BF)

    def down_parts(h, unit, cc):
        lo = 640 + 128 * h
        acts = jnp.concatenate([active[0:640, :], active[lo : lo + 128, :]], axis=0)
        mat = jnp.concatenate(
            [
                jnp.concatenate(
                    [g_d[h, 4 * place + 2 * cc + j], g_dt[0, 4 * place + 2 * cc + j]], axis=1
                )
                for place in order
                for j in range(2)
            ],
            axis=0,
        )
        term = dot(mat, acts).reshape(8, 64, 2 * SEQ)
        if cc is core:
            keep2[h] = term
        else:
            sb2[8 * h : 8 * h + 8] = term.astype(BF)
            for k in range(4):
                unit.part(k)

    own = cols_of(1, core)

    pack(0)
    ready("tok")
    pl.semaphore_wait(barrier, 7)
    s1(0)
    for s in range(2):
        gather_own(s, tfull, s)
    s1(1)
    s1(2)
    s2(0)
    s2(1)
    s3(0)
    gather_near(0, tfull, 0)
    tick(1)
    gather_near(1, tfull, 1)
    gather_far(0, tfull, 0)
    near_done(0, tfull, 0)
    add_squares(tfull, 0, (0, 3))
    tick(2)
    gather_far(1, tfull, 1)
    ready("mtaps", "ftaps")
    ahead(3)
    near_done(1, tfull, 1)
    add_squares(tfull, 1, (0, 3))
    for s in range(2):
        far_done(s, tfull, s)
        add_squares(tfull, s, (3, 4))
        row_factor(s)
    done(0)
    in_cgate()
    s4(2)
    ahead(4)
    done(1)
    in_value()
    s4(3)
    done(2)
    in_bgate()
    ahead(5)
    done(3)
    u0, u1 = mix_unit(0), mix_unit(1)
    mix_parts(0, u0)
    s4(4)
    s1(8)
    s2(7)
    u0.far()
    u0.near()
    s3(6)
    mix_parts(1, u1)
    s4(5)
    u1.far()
    u0.last()
    u1.near()
    s1(9)
    s2(8)
    s3(7)
    s4(6)
    s1(10)
    u1.last()
    s2(9)
    s1(11)
    s3(8)

    def residual(s, unit):
        unit.landed()
        for d in range(2):
            rows = slice(HALF * d, HALF * d + HALF)
            rfull[s, rows, own] = (tfull[s, rows, own].astype(F32) + unit.total(d)).astype(BF)
        gather_own(2 + s, rfull, s)

    residual(0, u0)
    s4(7)
    s2(10)
    residual(1, u1)
    s1(12)
    s3(9)
    s2(11)
    gather_near(2, rfull, 0)
    s4(8)
    s3(10)
    near_done(2, rfull, 0)
    add_squares(rfull, 0, (0, 3))
    for r in range(4, 8):
        done(r)
    s4(9)
    up_first(0, (0, 1, 2, 3))
    gather_near(3, rfull, 1)
    s3(11)
    s4(10)
    done(8)
    done(9)
    up_first(0, (4, 5))
    s2(12)
    gather_far(2, rfull, 0)
    near_done(3, rfull, 1)
    add_squares(rfull, 1, (0, 3))
    up_first(1, (0, 1, 2, 3, 4, 5))
    gather_far(3, rfull, 1)
    s4(11)

    def finish(s):
        far_done(2 + s, rfull, s)
        add_squares(rfull, s, (3, 4))
        row_factor(s)
        up_second(s)

    finish(0)
    s3(12)
    finish(1)
    done(10)
    done(11)
    v0, v1 = ffn_unit(0), ffn_unit(1)
    other = 1 - core
    down_parts(0, v0, other)
    s4(12)
    down_parts(0, v0, core)
    v0.far()
    v0.near()
    done(12)
    down_parts(1, v1, other)
    v0.last()
    down_parts(1, v1, core)
    v1.far()
    v1.near()
    v1.last()
    for src, ssem in sent:
        arrived(src, ssem)
    total = []
    for h, unit in enumerate((v0, v1)):
        unit.landed()
        total.append([unit.total(d) for d in range(2)])
    for s in range(2):
        for d in range(2):
            lanes = slice(SEQ * s, SEQ * s + SEQ)
            turned = jnp.concatenate([total[0][d][:, lanes], total[1][d][:, lanes]], axis=0).T
            cols = pl.ds(pl.multiple_of((2 + core) * W + 128 * d, 128), 128)
            out[s, :, 128 * d : 128 * d + 128] = (rfull[s, :, cols].astype(F32) + turned).astype(BF)


def on_device(
    tokens, mix_gain, w_bgate, w_cgate, w_value, in_scale, mix_taps, w_mixout, mixout_scale,
    ffn_gain, w_upgate, w_upval, up_scale, ffn_taps, w_down, down_scale,
):
    args = (
        tokens, mix_gain.reshape(16, 128), w_bgate, w_cgate, w_value, in_scale, mix_taps, w_mixout,
        mixout_scale, ffn_gain.reshape(16, 128), w_upgate.T, w_upval.T, up_scale,
        jnp.swapaxes(ffn_taps, 0, 1), w_down, down_scale,
    )
    vmem = pltpu.VMEM

    def exchange_buffers(piece, kept):
        return (
            vmem((16, *piece), BF),
            vmem((16, *piece), BF),
            vmem((2, *kept, *piece), F32),
            vmem((2, 2, *piece), BF),
            vmem((2, 2, 2, *piece), BF),
            vmem((2, 2, *piece), BF),
            vmem((2, 2, 2, *piece), BF),
        )

    dma = pltpu.SemaphoreType.DMA
    return pl.pallas_call(
        kernel,
        out_shape=jax.ShapeDtypeStruct(tokens.shape, BF),
        in_specs=[pl.BlockSpec(memory_space=pl.ANY)] * len(args),
        out_specs=pl.BlockSpec(memory_space=pltpu.VMEM),
        scratch_shapes=[
            *(vmem(a.shape, a.dtype) for a in args[1:]),
            vmem((3, 16, 128, W), BF),
            vmem((1, 16, 256, 128), BF),
            vmem((5, 16, 128, W), BF),
            vmem((1, 16, 128, 128), BF),
            vmem((1, 16, 64, 128), BF),
            vmem((2, 16, 64, 640), BF),
            vmem((2, SEQ, D), BF),
            vmem((2, SEQ, D), BF),
            vmem((2, SEQ, W), F32),
            vmem((2, SEQ, W), BF),
            vmem((896, 2 * SEQ), BF),
            vmem((2, SEQ, 128), F32),
            vmem((2, SEQ, 128), F32),
            vmem((2, 5, SEQ, W), F32),
            vmem((2, SEQ, 128), F32),
            *exchange_buffers((HALF, W), (4, 2)),
            *exchange_buffers((64, 2 * SEQ), (8,)),
            dma((ROUNDS,)),
            dma((ROUNDS, 7)),
            dma((4,)),
            dma((4, 5)),
            dma((4,)),
            dma((4, 4)),
            dma((16,)),
        ],
        compiler_params=pltpu.CompilerParams(
            collective_id=0, has_side_effects=True, vmem_limit_bytes=62 * 1024 * 1024
        ),
        name="layer",
    )(*args)


def solution(mesh):
    return jax.shard_map(
        on_device,
        mesh=mesh,
        in_specs=(
            P("fs", None, "tp"),
            P(),
            P("fs", "tp"),
            P("fs", "tp"),
            P("fs", "tp"),
            P(None, "tp"),
            P(None, "tp"),
            P("tp", "fs"),
            P(None, "fs"),
            P(),
            P("fs", "tp"),
            P("fs", "tp"),
            P(None, "tp"),
            P(None, None, "tp"),
            P("tp", "fs"),
            P(None, "fs"),
        ),
        out_specs=P("fs", None, "tp"),
        check_vma=False,
    )
```

```python
import functools

import jax
import jax.numpy as jnp
from jax import lax
from jax.experimental import pallas as pl
from jax.experimental.pallas import tpu as pltpu
from jax.sharding import PartitionSpec as P

EPS = 1e-06
BF = jnp.bfloat16
F32 = jnp.float32
SEQ = 384
HALF = SEQ // 2
D = 2048
W = 256
ROUNDS = 13


def kernel(
    tok_h, mgain_h, wb_h, wc_h, wv_h, insc_h, mtaps_h, wm_h, msc_h, fgain_h, wug_h, wuv_h, upsc_h, ftaps_h,
    wd_h, dsc_h,
    out,
    mgain, wb, wc, wv, insc, mtaps, wm, msc, fgain, wug, wuv, upsc, ftaps, wd, dsc,
    g_in, g_mo, g_up, g_ul, g_dt, g_d,
    tfull, rfull, cbuf, gated, active, fac, squares, acc, acc_tail,
    sb, rb, keep, fbuf, nbuf, rf, rn,
    sb2, rb2, keep2, fbuf2, nbuf2, rf2, rn2,
    y_send, y_recv, a_send, a_recv, r_send, r_recv, load_sem,
):
    fs = lax.axis_index("fs")
    tp = lax.axis_index("tp")
    z, y = fs // 4, fs % 4
    x, core = tp // 2, tp % 2
    xp, xm, xf = (x + 1) % 4, (x + 3) % 4, (x + 2) % 4
    dev_xp = (fs, xp * 2 + core)
    dev_xm = (fs, xm * 2 + core)
    dev_sib = (fs, x * 2 + 1 - core)
    dev_axis = (
        ((z * 4 + (y + 1) % 4, tp), (z * 4 + (y + 3) % 4, tp)),
        ((((z + 1) % 4) * 4 + y, tp), (((z + 3) % 4) * 4 + y, tp)),
    )
    pos = (y, z)
    sent = []

    def slot(zz):
        return (zz - x + 5) % 4


    def push(src, dst, ssem, rsem, dev):
        pltpu.make_async_remote_copy(
            src_ref=src, dst_ref=dst, send_sem=ssem, recv_sem=rsem,
            device_id=dev, device_id_type=pl.DeviceIdType.MESH,
        ).start()

    def arrived(dst, rsem):
        pltpu.make_async_copy(dst, dst, rsem).wait()

    barrier = pltpu.get_barrier_semaphore()
    for dev in (*dev_axis[0], *dev_axis[1], dev_xp, dev_xm, dev_sib):
        pl.semaphore_signal(barrier, inc=1, device_id=dev, device_id_type=pl.DeviceIdType.MESH)

    loads = {}

    def load(name, src, dst):
        loads[name] = pltpu.make_async_copy(src, dst, load_sem.at[len(loads)])
        loads[name].start()

    def cols_of(place, cc):
        return pl.ds(pl.multiple_of((place * 2 + cc) * W, W), W)

    load("tok", tok_h, tfull.at[:, :, cols_of(1, core)])
    for name, src, dst in (
        ("wc", wc_h, wc), ("mgain", mgain_h, mgain), ("insc", insc_h, insc), ("wv", wv_h, wv), ("wb", wb_h, wb),
        ("msc", msc_h, msc), ("wm", wm_h, wm), ("fgain", fgain_h, fgain), ("upsc", upsc_h, upsc),
        ("wug", wug_h, wug), ("wuv", wuv_h, wuv), ("dsc", dsc_h, dsc), ("wd", wd_h, wd),
        ("mtaps", mtaps_h, mtaps), ("ftaps", ftaps_h, ftaps),
    ):
        load(name, src, dst)

    def ready(*names):
        for name in names:
            if name in loads:
                loads.pop(name).wait()

    def rounded(w):
        return w.astype(BF).astype(F32)

    tail = slice(640, 704)

    mine = slot(z) * 4 + y

    def pack(r):
        if r < 3:
            w, row = ((wc, 1), (wv, 2), (wb, 0))[r]
            ready("mgain", "insc", ("wc", "wv", "wb")[r])
            col = jnp.broadcast_to(mgain[pl.ds(fs, 1), :], (128, 128)).T
            col = jnp.concatenate([col, col], axis=1)
            g_in[r, mine] = (rounded(w[...]) * col * insc[row : row + 1, :]).astype(BF)
        elif r == 3:
            ready("msc", "wm")
            g_mo[0, mine] = (rounded(wm[...]) * msc[...]).astype(BF)
        elif r < 9:
            ready("fgain", "upsc", "wug", "wuv")
            frow = fgain[pl.ds(fs, 1), :]
            j = r - 4
            cols = slice(128 * j, 128 * j + 128)
            for k, w in enumerate((wug, wuv)):
                g_up[j, mine, :, 128 * k : 128 * k + 128] = (
                    (rounded(w[cols, :]) * frow).T * upsc[k : k + 1, cols]
                ).astype(BF)
        elif r == 9:
            frow = fgain[pl.ds(fs, 1), :]
            both = rounded(jnp.concatenate([wug[tail, :], wuv[tail, :]], axis=0))
            tail_scale = jnp.concatenate([upsc[0:1, tail], upsc[1:2, tail]], axis=1)
            g_ul[0, mine] = ((both * frow).T * tail_scale).astype(BF)
        elif r == 10:
            ready("dsc", "wd")
            last = rounded(wd[tail, :]) * dsc[...]
            turned = jnp.concatenate([last, last], axis=0).T
            lane = lax.broadcasted_iota(jnp.int32, (64, 128), 1)
            g_dt[0, mine] = jnp.where(lane < 64, turned[0:64], turned[64:128]).astype(BF)
        elif r < 13:
            lo = 64 * (r - 11)
            for j in range(5):
                cols = slice(128 * j, 128 * j + 128)
                turned = (rounded(wd[cols, :]) * dsc[...]).T
                g_d[r - 11, mine, :, cols] = turned[lo : lo + 64].astype(BF)

    rounds = (
        [(g_in, k, 128) for k in range(3)]
        + [(g_mo, 0, 256)]
        + [(g_up, k, 128) for k in range(5)]
        + [(g_ul, 0, 128), (g_dt, 0, 64)]
        + [(g_d, k, 64) for k in range(2)]
    )

    def block(r, h, p_at, q_at, lo, n):
        ref, k, rows = rounds[r]
        zz, yy = (q_at, p_at) if h == 0 else (p_at, q_at)
        return ref.at[k, slot(zz) * 4 + yy, pl.ds(lo, n), :]

    def some(r, n, rows):
        ref, k, _ = rounds[r]
        return ref.at[k, pl.ds(0, n), pl.ds(0, rows), :]

    def geometry(r, h):
        half = rounds[r][2] // 2
        lo = half * h
        return lo, half, lo, lo + half // 2, half // 2, pos[h], pos[1 - h]

    def hop(r, h, stage, piece, axis, d):
        push(piece, piece, y_send.at[r], y_recv.at[r, 2 * stage + h if stage < 3 else 6], dev_axis[axis][d])

    def across(r, h, p_at):
        lo, half, up, dn, quarter, p, q = geometry(r, h)
        for d in range(2):
            hop(r, h, 2, block(r, h, p_at, q, lo, half), 1 - h, d)

    def s1(r):
        if not 0 <= r < ROUNDS:
            return
        pack(r + 1)
        for h in range(2):
            lo, half, up, dn, quarter, p, q = geometry(r, h)
            for d in range(2):
                hop(r, h, 0, block(r, h, p, q, lo, half), h, d)
            across(r, h, p)

    def s2(r):
        if not 0 <= r < ROUNDS:
            return
        for h in range(2):
            lo, half, up, dn, quarter, p, q = geometry(r, h)
            arrived(some(r, 2, half), y_recv.at[r, h])
            for d, at, part in ((0, (p + 3) % 4, up), (1, (p + 1) % 4, dn)):
                hop(r, h, 1, block(r, h, at, q, part, quarter), h, d)
            for at in ((p + 3) % 4, (p + 1) % 4):
                across(r, h, at)

    def s3(r):
        if not 0 <= r < ROUNDS:
            return
        for h in range(2):
            lo, half, up, dn, quarter, p, q = geometry(r, h)
            arrived(some(r, 2, quarter), y_recv.at[r, 2 + h])
            across(r, h, (p + 2) % 4)

    def s4(r):
        if not 0 <= r < ROUNDS:
            return
        for h in range(2):
            lo, half, up, dn, quarter, p, q = geometry(r, h)
            arrived(some(r, 8, half), y_recv.at[r, 4 + h])
            for d, at, part in ((0, (q + 3) % 4, up), (1, (q + 1) % 4, dn)):
                for k in range(4):
                    hop(r, h, 3, block(r, h, k, at, part, quarter), 1 - h, d)
        sent.append((some(r, 15, rounds[r][2]), y_send.at[r]))

    def done(r):
        arrived(some(r, 16, rounds[r][2] // 4), y_recv.at[r, 6])

    def ahead(k):
        s1(k + 2)
        s2(k + 1)
        s3(k)

    def tick(k):
        ahead(k)
        s4(k - 1)

    def gather_own(u, buf, s):
        src = buf.at[s, :, cols_of(1, core)]
        push(src, buf.at[s, :, cols_of(0, core)], a_send.at[u], a_recv.at[u, 0], dev_xp)
        push(src, buf.at[s, :, cols_of(2, core)], a_send.at[u], a_recv.at[u, 1], dev_xm)
        push(src, src, a_send.at[u], a_recv.at[u, 3], dev_sib)

    def gather_near(u, buf, s):
        for d, place, lo, dev in ((0, 0, 0, dev_xp), (1, 2, HALF, dev_xm)):
            whole = buf.at[s, :, cols_of(place, core)]
            arrived(whole, a_recv.at[u, d])
            rows = pl.ds(lo, HALF)
            push(
                buf.at[s, rows, cols_of(place, core)], buf.at[s, rows, cols_of(3, core)],
                a_send.at[u], a_recv.at[u, 2], dev,
            )
            push(whole, whole, a_send.at[u], a_recv.at[u, 3], dev_sib)

    def gather_far(u, buf, s):
        whole = buf.at[s, :, cols_of(3, core)]
        arrived(whole, a_recv.at[u, 2])
        push(whole, whole, a_send.at[u], a_recv.at[u, 4], dev_sib)
        sent.append((sb.at[pl.ds(0, 14)], a_send.at[u]))

    def near_done(u, buf, s):
        arrived(buf.at[s, :, pl.ds(0, 3 * W)], a_recv.at[u, 3])

    def far_done(u, buf, s):
        arrived(buf.at[s, :, cols_of(3, 1 - core)], a_recv.at[u, 4])

    def add_squares(buf, s, places):
        total = None
        for j in range(4 * places[0], 4 * places[1]):
            v = buf[s, :, 128 * j : 128 * j + 128].astype(F32)
            total = v * v if total is None else total + v * v
        squares[s] = total if places[0] == 0 else squares[s] + total

    def row_factor(s):
        mean = jnp.sum(squares[s], axis=1, keepdims=True) * (1.0 / D)
        fac[s] = jnp.broadcast_to(lax.rsqrt(mean + EPS), (SEQ, 128))

    def shifted(v, n):
        turned = pltpu.roll(v, n, 0)
        row = lax.broadcasted_iota(jnp.int32, (8, v.shape[1]), 0)
        return jnp.concatenate([jnp.where(row >= n, turned[0:8], 0.0), turned[8:]], axis=0)

    def causal(v, taps):
        return shifted(v, 2) * taps[0:1] + shifted(v, 1) * taps[1:2] + v * taps[2:3]

    def wide(s):
        f = fac[s]
        return jnp.concatenate([f, f], axis=1)

    order = (3, 2, 0, 1)

    class Unit:
        def __init__(self, u, sems, sb, rb, keep, fbuf, nbuf, rf, rn):
            self.fbuf, self.nbuf, self.rf, self.rn = (ref.at[u] for ref in (fbuf, nbuf, rf, rn))
            self.sb, self.rb, self.base = sb, rb, 8 * u
            self.keep = keep
            self.ssem, self.rsem = r_send.at[sems], r_recv.at[sems]

        def pieces(self, ref, k, n=1):
            return ref.at[pl.ds(self.base + 2 * k, 2 * n)]

        def part(self, k):
            push(
                self.pieces(self.sb, k), self.pieces(self.rb, k),
                self.ssem, self.rsem.at[(0, 1, 1, 3)[k]], dev_sib,
            )

        def both(self, k, d):
            return self.keep(k, d) + self.rb[self.base + 2 * k + d].astype(F32)

        def far(self):
            arrived(self.pieces(self.rb, 0), self.rsem.at[0])
            for d in range(2):
                self.fbuf[d] = self.both(0, d).astype(BF)
            for d, dev in ((0, dev_xp), (1, dev_xm)):
                push(self.fbuf.at[d], self.rf.at[d], self.ssem, self.rsem.at[2], dev)

        def near(self):
            arrived(self.pieces(self.rb, 1, 2), self.rsem.at[1])
            for d in range(2):
                self.nbuf[d, 1 - d] = self.both(1 + d, 1 - d).astype(BF)
            for d, dev in ((0, dev_xp), (1, dev_xm)):
                push(self.nbuf.at[d, 1 - d], self.rn.at[d, 1 - d], self.ssem, self.rsem.at[3], dev)

        def last(self):
            arrived(self.rf, self.rsem.at[2])
            for d in range(2):
                self.nbuf[d, d] = (self.both(1 + d, d) + self.rf[d].astype(F32)).astype(BF)
            for d, dev in ((0, dev_xp), (1, dev_xm)):
                push(self.nbuf.at[d, d], self.rn.at[d, d], self.ssem, self.rsem.at[3], dev)
            sent.append((sb.at[pl.ds(0, 14)], self.ssem))

        def landed(self):
            arrived(self.rb.at[pl.ds(0, 6)], self.rsem.at[3])

        def total(self, d):
            return self.both(3, d) + self.rn[0, d].astype(F32) + self.rn[1, d].astype(F32)

    def mix_unit(s):
        return Unit(s, s, sb, rb, lambda k, d: keep[s, k, d], fbuf, nbuf, rf, rn)

    def ffn_unit(h):
        return Unit(
            h, 2 + h, sb2, rb2, lambda k, d: keep2[h, 2 * k + d], fbuf2, nbuf2, rf2, rn2
        )

    def dot(a, b):
        return jnp.dot(a, b, preferred_element_type=F32)

    def in_cgate():
        @pl.loop(0, 2)
        def _(s):
            cbuf[s] = dot(tfull[s], g_in[0].reshape(D, W))

    def in_value():
        @pl.loop(0, 2)
        def _(s):
            f = wide(s)
            inner = dot(tfull[s], g_in[1].reshape(D, W)) * cbuf[s] * (f * f)
            cbuf[s] = causal(inner, mtaps) * f

    def in_bgate():
        @pl.loop(0, 2)
        def _(s):
            gated[s] = (dot(tfull[s], g_in[2].reshape(D, W)) * cbuf[s]).astype(BF)

    def mix_parts(s, unit):
        for cc in (1 - core, core):
            mat = jnp.concatenate([g_mo[0, 4 * place + 2 * cc + j] for place in order for j in range(2)], axis=1)
            term = dot(gated[s], mat)
            for k in range(4):
                piece = term[:, W * k : W * k + W].reshape(2, HALF, W)
                if cc is core:
                    keep[s, k] = piece
                else:
                    sb[8 * s + 2 * k : 8 * s + 2 * k + 2] = piece.astype(BF)
                    unit.part(k)

    def up_first(s, js):
        for j in js:
            if j < 5:
                acc[s, j] = dot(rfull[s, :, 0:1536], g_up[j, 0:12].reshape(1536, W))
            else:
                acc_tail[s] = dot(rfull[s, :, 0:1536], g_ul[0, 0:12].reshape(1536, 128))

    def tokens_of(s):
        return slice(SEQ * s, SEQ * s + SEQ)

    def silu(v):
        return v / (1.0 + jnp.exp(-v))

    def up_second(s):
        for j in range(5):
            cols = slice(128 * j, 128 * j + 128)
            pre = (acc[s, j] + dot(rfull[s, :, 1536:2048], g_up[j, 12:16].reshape(512, W))) * wide(s)
            taps = jnp.concatenate([ftaps[:, 0, cols], ftaps[:, 1, cols]], axis=1)
            conv = causal(pre, taps)
            active[cols, tokens_of(s)] = (silu(conv[:, 0:128]) * conv[:, 128:256]).T.astype(BF)
        pre = (acc_tail[s] + dot(rfull[s, :, 1536:2048], g_ul[0, 12:16].reshape(512, 128))) * fac[s]
        taps = jnp.concatenate([ftaps[:, 0, tail], ftaps[:, 1, tail]], axis=1)
        conv = causal(pre, taps)
        act = (silu(conv) * pltpu.roll(conv, 64, 1)).T[0:64].astype(BF)
        active[640:704, tokens_of(s)] = act
        active[832:896, tokens_of(s)] = act
        active[704:832, tokens_of(s)] = jnp.zeros((128, SEQ), BF)

    def down_parts(h, unit, cc):
        lo = 640 + 128 * h
        acts = jnp.concatenate([active[0:640, :], active[lo : lo + 128, :]], axis=0)
        mat = jnp.concatenate(
            [
                jnp.concatenate(
                    [g_d[h, 4 * place + 2 * cc + j], g_dt[0, 4 * place + 2 * cc + j]], axis=1
                )
                for place in order
                for j in range(2)
            ],
            axis=0,
        )
        term = dot(mat, acts).reshape(8, 64, 2 * SEQ)
        if cc is core:
            keep2[h] = term
        else:
            sb2[8 * h : 8 * h + 8] = term.astype(BF)
            for k in range(4):
                unit.part(k)

    own = cols_of(1, core)

    pack(0)
    ready("tok")
    pl.semaphore_wait(barrier, 7)
    s1(0)
    for s in range(2):
        gather_own(s, tfull, s)
    s1(1)
    s1(2)
    s2(0)
    s2(1)
    s3(0)
    gather_near(0, tfull, 0)
    tick(1)
    gather_near(1, tfull, 1)
    gather_far(0, tfull, 0)
    near_done(0, tfull, 0)
    add_squares(tfull, 0, (0, 3))
    tick(2)
    gather_far(1, tfull, 1)
    ready("mtaps", "ftaps")
    ahead(3)
    near_done(1, tfull, 1)
    add_squares(tfull, 1, (0, 3))
    for s in range(2):
        far_done(s, tfull, s)
        add_squares(tfull, s, (3, 4))
        row_factor(s)
    done(0)
    in_cgate()
    s4(2)
    ahead(4)
    done(1)
    in_value()
    s4(3)
    done(2)
    in_bgate()
    ahead(5)
    done(3)
    u0, u1 = mix_unit(0), mix_unit(1)
    mix_parts(0, u0)
    s4(4)
    s1(8)
    s2(7)
    u0.far()
    u0.near()
    s3(6)
    mix_parts(1, u1)
    s4(5)
    s1(9)
    s1(10)
    u1.far()
    s2(8)
    u0.last()
    u1.near()
    s3(7)
    s4(6)
    s1(11)
    s2(9)
    u1.last()
    s3(8)
    s2(10)

    def residual(s, unit):
        unit.landed()
        for d in range(2):
            rows = slice(HALF * d, HALF * d + HALF)
            rfull[s, rows, own] = (tfull[s, rows, own].astype(F32) + unit.total(d)).astype(BF)
        gather_own(2 + s, rfull, s)

    residual(0, u0)
    s4(7)
    s1(12)
    residual(1, u1)
    s3(9)
    s2(11)
    s3(10)
    gather_near(2, rfull, 0)
    s4(8)
    near_done(2, rfull, 0)
    add_squares(rfull, 0, (0, 3))
    for r in range(4, 8):
        done(r)
    s4(9)
    s2(12)
    up_first(0, (0, 1, 2, 3))
    s3(11)
    gather_near(3, rfull, 1)
    s4(10)
    done(8)
    done(9)
    up_first(0, (4, 5))
    gather_far(2, rfull, 0)
    s3(12)
    near_done(3, rfull, 1)
    add_squares(rfull, 1, (0, 3))
    up_first(1, (0, 1, 2, 3, 4, 5))
    s4(11)
    gather_far(3, rfull, 1)

    def finish(s):
        far_done(2 + s, rfull, s)
        add_squares(rfull, s, (3, 4))
        row_factor(s)
        up_second(s)

    finish(0)
    finish(1)
    s4(12)
    done(10)
    done(11)
    v0, v1 = ffn_unit(0), ffn_unit(1)
    other = 1 - core
    down_parts(0, v0, other)
    down_parts(0, v0, core)
    v0.far()
    v0.near()
    done(12)
    down_parts(1, v1, other)
    down_parts(1, v1, core)
    v1.far()
    v0.last()
    v1.near()
    v1.last()
    for src, ssem in sent:
        arrived(src, ssem)
    total = []
    for h, unit in enumerate((v0, v1)):
        unit.landed()
        total.append([unit.total(d) for d in range(2)])
    for s in range(2):
        for d in range(2):
            lanes = slice(SEQ * s, SEQ * s + SEQ)
            turned = jnp.concatenate([total[0][d][:, lanes], total[1][d][:, lanes]], axis=0).T
            cols = pl.ds(pl.multiple_of((2 + core) * W + 128 * d, 128), 128)
            out[s, :, 128 * d : 128 * d + 128] = (rfull[s, :, cols].astype(F32) + turned).astype(BF)


def on_device(
    tokens, mix_gain, w_bgate, w_cgate, w_value, in_scale, mix_taps, w_mixout, mixout_scale,
    ffn_gain, w_upgate, w_upval, up_scale, ffn_taps, w_down, down_scale,
):
    args = (
        tokens, mix_gain.reshape(16, 128), w_bgate, w_cgate, w_value, in_scale, mix_taps, w_mixout,
        mixout_scale, ffn_gain.reshape(16, 128), w_upgate.T, w_upval.T, up_scale,
        jnp.swapaxes(ffn_taps, 0, 1), w_down, down_scale,
    )
    vmem = pltpu.VMEM

    def exchange_buffers(piece, kept):
        return (
            vmem((16, *piece), BF),
            vmem((16, *piece), BF),
            vmem((2, *kept, *piece), F32),
            vmem((2, 2, *piece), BF),
            vmem((2, 2, 2, *piece), BF),
            vmem((2, 2, *piece), BF),
            vmem((2, 2, 2, *piece), BF),
        )

    dma = pltpu.SemaphoreType.DMA
    return pl.pallas_call(
        kernel,
        out_shape=vmem(tokens.shape, BF),
        in_specs=[pl.BlockSpec(memory_space=pl.ANY)] * len(args),
        out_specs=pl.BlockSpec(memory_space=pltpu.VMEM),
        scratch_shapes=[
            *(vmem(a.shape, a.dtype) for a in args[1:]),
            vmem((3, 16, 128, W), BF),
            vmem((1, 16, 256, 128), BF),
            vmem((5, 16, 128, W), BF),
            vmem((1, 16, 128, 128), BF),
            vmem((1, 16, 64, 128), BF),
            vmem((2, 16, 64, 640), BF),
            vmem((2, SEQ, D), BF),
            vmem((2, SEQ, D), BF),
            vmem((2, SEQ, W), F32),
            vmem((2, SEQ, W), BF),
            vmem((896, 2 * SEQ), BF),
            vmem((2, SEQ, 128), F32),
            vmem((2, SEQ, 128), F32),
            vmem((2, 5, SEQ, W), F32),
            vmem((2, SEQ, 128), F32),
            *exchange_buffers((HALF, W), (4, 2)),
            *exchange_buffers((64, 2 * SEQ), (8,)),
            dma((ROUNDS,)),
            dma((ROUNDS, 7)),
            dma((4,)),
            dma((4, 5)),
            dma((4,)),
            dma((4, 4)),
            dma((16,)),
        ],
        compiler_params=pltpu.CompilerParams(
            collective_id=0, has_side_effects=True, vmem_limit_bytes=60 * 1024 * 1024
        ),
        name="layer",
    )(*args)


def solution(mesh):
    return jax.shard_map(
        on_device,
        mesh=mesh,
        in_specs=(
            P("fs", None, "tp"),
            P(),
            P("fs", "tp"),
            P("fs", "tp"),
            P("fs", "tp"),
            P(None, "tp"),
            P(None, "tp"),
            P("tp", "fs"),
            P(None, "fs"),
            P(),
            P("fs", "tp"),
            P("fs", "tp"),
            P(None, "tp"),
            P(None, None, "tp"),
            P("tp", "fs"),
            P(None, "fs"),
        ),
        out_specs=P("fs", None, "tp"),
        check_vma=False,
    )
```

```python
import functools

import jax
import jax.numpy as jnp
from jax import lax
from jax.experimental import pallas as pl
from jax.experimental.pallas import tpu as pltpu
from jax.sharding import PartitionSpec as P

EPS = 1e-06
BF = jnp.bfloat16
F32 = jnp.float32
SEQ = 384
HALF = SEQ // 2
D = 2048
W = 256
ROUNDS = 13


def kernel(
    tok_h, mgain_h, wb_h, wc_h, wv_h, insc_h, mtaps_h, wm_h, msc_h, fgain_h, wug_h, wuv_h, upsc_h, ftaps_h,
    wd_h, dsc_h,
    out,
    mgain, wb, wc, wv, insc, mtaps, wm, msc, fgain, wug, wuv, upsc, ftaps, wd, dsc,
    g_in, g_mo, g_up, g_ul, g_dt, g_d,
    tfull, rfull, cbuf, gated, active, fac, squares, acc, acc_tail,
    sb, rb, keep, fbuf, nbuf, rf, rn,
    sb2, rb2, keep2, fbuf2, nbuf2, rf2, rn2,
    y_send, y_recv, a_send, a_recv, r_send, r_recv, load_sem,
):
    fs = lax.axis_index("fs")
    tp = lax.axis_index("tp")
    z, y = fs // 4, fs % 4
    x, core = tp // 2, tp % 2
    xp, xm, xf = (x + 1) % 4, (x + 3) % 4, (x + 2) % 4
    dev_xp = (fs, xp * 2 + core)
    dev_xm = (fs, xm * 2 + core)
    dev_sib = (fs, x * 2 + 1 - core)
    dev_axis = (
        ((z * 4 + (y + 1) % 4, tp), (z * 4 + (y + 3) % 4, tp)),
        ((((z + 1) % 4) * 4 + y, tp), (((z + 3) % 4) * 4 + y, tp)),
    )
    pos = (y, z)
    sent = []

    def slot(zz):
        return (zz - x + 5) % 4


    def push(src, dst, ssem, rsem, dev):
        pltpu.make_async_remote_copy(
            src_ref=src, dst_ref=dst, send_sem=ssem, recv_sem=rsem,
            device_id=dev, device_id_type=pl.DeviceIdType.MESH,
        ).start()

    def arrived(dst, rsem):
        pltpu.make_async_copy(dst, dst, rsem).wait()

    barrier = pltpu.get_barrier_semaphore()
    for dev in (*dev_axis[0], *dev_axis[1], dev_xp, dev_xm, dev_sib):
        pl.semaphore_signal(barrier, inc=1, device_id=dev, device_id_type=pl.DeviceIdType.MESH)

    loads = {}

    def load(name, src, dst):
        loads[name] = pltpu.make_async_copy(src, dst, load_sem.at[len(loads)])
        loads[name].start()

    def cols_of(place, cc):
        return pl.ds(pl.multiple_of((place * 2 + cc) * W, W), W)

    load("tok", tok_h, tfull.at[:, :, cols_of(1, core)])
    for name, src, dst in (
        ("wc", wc_h, wc), ("mgain", mgain_h, mgain), ("insc", insc_h, insc), ("wv", wv_h, wv), ("wb", wb_h, wb),
        ("msc", msc_h, msc), ("wm", wm_h, wm), ("fgain", fgain_h, fgain), ("upsc", upsc_h, upsc),
        ("wug", wug_h, wug), ("wuv", wuv_h, wuv), ("dsc", dsc_h, dsc), ("wd", wd_h, wd),
        ("mtaps", mtaps_h, mtaps), ("ftaps", ftaps_h, ftaps),
    ):
        load(name, src, dst)

    def ready(*names):
        for name in names:
            if name in loads:
                loads.pop(name).wait()

    def rounded(w):
        return w.astype(BF).astype(F32)

    tail = slice(640, 704)

    mine = slot(z) * 4 + y

    def pack(r):
        if r < 3:
            w, row = ((wc, 1), (wv, 2), (wb, 0))[r]
            ready("mgain", "insc", ("wc", "wv", "wb")[r])
            col = jnp.broadcast_to(mgain[pl.ds(fs, 1), :], (128, 128)).T
            col = jnp.concatenate([col, col], axis=1)
            g_in[r, mine] = (rounded(w[...]) * col * insc[row : row + 1, :]).astype(BF)
        elif r == 3:
            ready("msc", "wm")
            g_mo[0, mine] = (rounded(wm[...]) * msc[...]).astype(BF)
        elif r < 9:
            ready("fgain", "upsc", "wug", "wuv")
            frow = fgain[pl.ds(fs, 1), :]
            j = r - 4
            cols = slice(128 * j, 128 * j + 128)
            for k, w in enumerate((wug, wuv)):
                g_up[j, mine, :, 128 * k : 128 * k + 128] = (
                    (rounded(w[cols, :]) * frow).T * upsc[k : k + 1, cols]
                ).astype(BF)
        elif r == 9:
            frow = fgain[pl.ds(fs, 1), :]
            both = rounded(jnp.concatenate([wug[tail, :], wuv[tail, :]], axis=0))
            tail_scale = jnp.concatenate([upsc[0:1, tail], upsc[1:2, tail]], axis=1)
            g_ul[0, mine] = ((both * frow).T * tail_scale).astype(BF)
        elif r == 10:
            ready("dsc", "wd")
            last = rounded(wd[tail, :]) * dsc[...]
            turned = jnp.concatenate([last, last], axis=0).T
            lane = lax.broadcasted_iota(jnp.int32, (64, 128), 1)
            g_dt[0, mine] = jnp.where(lane < 64, turned[0:64], turned[64:128]).astype(BF)
        elif r < 13:
            lo = 64 * (r - 11)
            for j in range(5):
                cols = slice(128 * j, 128 * j + 128)
                turned = (rounded(wd[cols, :]) * dsc[...]).T
                g_d[r - 11, mine, :, cols] = turned[lo : lo + 64].astype(BF)

    rounds = (
        [(g_in, k, 128) for k in range(3)]
        + [(g_mo, 0, 256)]
        + [(g_up, k, 128) for k in range(5)]
        + [(g_ul, 0, 128), (g_dt, 0, 64)]
        + [(g_d, k, 64) for k in range(2)]
    )

    def block(r, h, p_at, q_at, lo, n):
        ref, k, rows = rounds[r]
        zz, yy = (q_at, p_at) if h == 0 else (p_at, q_at)
        return ref.at[k, slot(zz) * 4 + yy, pl.ds(lo, n), :]

    def some(r, n, rows):
        ref, k, _ = rounds[r]
        return ref.at[k, pl.ds(0, n), pl.ds(0, rows), :]

    def geometry(r, h):
        half = rounds[r][2] // 2
        lo = half * h
        return lo, half, lo, lo + half // 2, half // 2, pos[h], pos[1 - h]

    def hop(r, h, stage, piece, axis, d):
        push(piece, piece, y_send.at[r], y_recv.at[r, stage], dev_axis[axis][d])

    def across(r, h, p_at):
        lo, half, up, dn, quarter, p, q = geometry(r, h)
        for d in range(2):
            hop(r, h, 2, block(r, h, p_at, q, lo, half), 1 - h, d)

    def s1(r):
        if not 0 <= r < ROUNDS:
            return
        pack(r + 1)
        for h in range(2):
            lo, half, up, dn, quarter, p, q = geometry(r, h)
            for d in range(2):
                hop(r, h, 0, block(r, h, p, q, lo, half), h, d)
            across(r, h, p)

    def s2(r):
        if not 0 <= r < ROUNDS:
            return
        arrived(some(r, 4, rounds[r][2] // 2), y_recv.at[r, 0])
        for h in range(2):
            lo, half, up, dn, quarter, p, q = geometry(r, h)
            for d, at, part in ((0, (p + 3) % 4, up), (1, (p + 1) % 4, dn)):
                hop(r, h, 1, block(r, h, at, q, part, quarter), h, d)
        for h in range(2):
            lo, half, up, dn, quarter, p, q = geometry(r, h)
            for at in ((p + 3) % 4, (p + 1) % 4):
                across(r, h, at)

    def s3(r):
        if not 0 <= r < ROUNDS:
            return
        arrived(some(r, 4, rounds[r][2] // 4), y_recv.at[r, 1])
        for h in range(2):
            across(r, h, (pos[h] + 2) % 4)

    def s4(r):
        if not 0 <= r < ROUNDS:
            return
        arrived(some(r, 16, rounds[r][2] // 2), y_recv.at[r, 2])
        for h in range(2):
            lo, half, up, dn, quarter, p, q = geometry(r, h)
            for d, at, part in ((0, (q + 3) % 4, up), (1, (q + 1) % 4, dn)):
                for k in range(4):
                    hop(r, h, 3, block(r, h, k, at, part, quarter), 1 - h, d)
        sent.append((some(r, 15, rounds[r][2]), y_send.at[r]))

    def done(r):
        arrived(some(r, 16, rounds[r][2] // 4), y_recv.at[r, 3])

    def ahead(k):
        s1(k + 2)
        s2(k + 1)
        s3(k)

    def tick(k):
        ahead(k)
        s4(k - 1)

    def gather_own(u, buf, s):
        src = buf.at[s, :, cols_of(1, core)]
        push(src, buf.at[s, :, cols_of(0, core)], a_send.at[u], a_recv.at[u, 0], dev_xp)
        push(src, buf.at[s, :, cols_of(2, core)], a_send.at[u], a_recv.at[u, 1], dev_xm)
        push(src, src, a_send.at[u], a_recv.at[u, 3], dev_sib)

    def gather_near(u, buf, s):
        for d, place, lo, dev in ((0, 0, 0, dev_xp), (1, 2, HALF, dev_xm)):
            whole = buf.at[s, :, cols_of(place, core)]
            arrived(whole, a_recv.at[u, d])
            rows = pl.ds(lo, HALF)
            push(
                buf.at[s, rows, cols_of(place, core)], buf.at[s, rows, cols_of(3, core)],
                a_send.at[u], a_recv.at[u, 2], dev,
            )
            push(whole, whole, a_send.at[u], a_recv.at[u, 3], dev_sib)

    def gather_far(u, buf, s):
        whole = buf.at[s, :, cols_of(3, core)]
        arrived(whole, a_recv.at[u, 2])
        push(whole, whole, a_send.at[u], a_recv.at[u, 4], dev_sib)
        sent.append((sb.at[pl.ds(0, 14)], a_send.at[u]))

    def near_done(u, buf, s):
        arrived(buf.at[s, :, pl.ds(0, 3 * W)], a_recv.at[u, 3])

    def far_done(u, buf, s):
        arrived(buf.at[s, :, cols_of(3, 1 - core)], a_recv.at[u, 4])

    def add_squares(buf, s, places):
        total = None
        for j in range(4 * places[0], 4 * places[1]):
            v = buf[s, :, 128 * j : 128 * j + 128].astype(F32)
            total = v * v if total is None else total + v * v
        squares[s] = total if places[0] == 0 else squares[s] + total

    def row_factor(s):
        mean = jnp.sum(squares[s], axis=1, keepdims=True) * (1.0 / D)
        fac[s] = jnp.broadcast_to(lax.rsqrt(mean + EPS), (SEQ, 128))

    def shifted(v, n):
        turned = pltpu.roll(v, n, 0)
        row = lax.broadcasted_iota(jnp.int32, (8, v.shape[1]), 0)
        return jnp.concatenate([jnp.where(row >= n, turned[0:8], 0.0), turned[8:]], axis=0)

    def causal(v, taps):
        return shifted(v, 2) * taps[0:1] + shifted(v, 1) * taps[1:2] + v * taps[2:3]

    def wide(s):
        f = fac[s]
        return jnp.concatenate([f, f], axis=1)

    order = (3, 2, 0, 1)

    class Unit:
        def __init__(self, u, sems, sb, rb, keep, fbuf, nbuf, rf, rn):
            self.fbuf, self.nbuf, self.rf, self.rn = (ref.at[u] for ref in (fbuf, nbuf, rf, rn))
            self.sb, self.rb, self.base = sb, rb, 8 * u
            self.keep = keep
            self.ssem, self.rsem = r_send.at[sems], r_recv.at[sems]

        def pieces(self, ref, k, n=1):
            return ref.at[pl.ds(self.base + 2 * k, 2 * n)]

        def part(self, k):
            push(
                self.pieces(self.sb, k), self.pieces(self.rb, k),
                self.ssem, self.rsem.at[(0, 1, 1, 3)[k]], dev_sib,
            )

        def both(self, k, d):
            return self.keep(k, d) + self.rb[self.base + 2 * k + d].astype(F32)

        def far(self):
            arrived(self.pieces(self.rb, 0), self.rsem.at[0])
            for d in range(2):
                self.fbuf[d] = self.both(0, d).astype(BF)
            for d, dev in ((0, dev_xp), (1, dev_xm)):
                push(self.fbuf.at[d], self.rf.at[d], self.ssem, self.rsem.at[2], dev)

        def near(self):
            arrived(self.pieces(self.rb, 1, 2), self.rsem.at[1])
            for d in range(2):
                self.nbuf[d, 1 - d] = self.both(1 + d, 1 - d).astype(BF)
            for d, dev in ((0, dev_xp), (1, dev_xm)):
                push(self.nbuf.at[d, 1 - d], self.rn.at[d, 1 - d], self.ssem, self.rsem.at[3], dev)

        def last(self):
            arrived(self.rf, self.rsem.at[2])
            for d in range(2):
                self.nbuf[d, d] = (self.both(1 + d, d) + self.rf[d].astype(F32)).astype(BF)
            for d, dev in ((0, dev_xp), (1, dev_xm)):
                push(self.nbuf.at[d, d], self.rn.at[d, d], self.ssem, self.rsem.at[3], dev)
            sent.append((sb.at[pl.ds(0, 14)], self.ssem))

        def landed(self):
            arrived(self.rb.at[pl.ds(0, 6)], self.rsem.at[3])

        def total(self, d):
            return self.both(3, d) + self.rn[0, d].astype(F32) + self.rn[1, d].astype(F32)

    def mix_unit(s):
        return Unit(s, s, sb, rb, lambda k, d: keep[s, k, d], fbuf, nbuf, rf, rn)

    def ffn_unit(h):
        return Unit(
            h, 2 + h, sb2, rb2, lambda k, d: keep2[h, 2 * k + d], fbuf2, nbuf2, rf2, rn2
        )

    def dot(a, b):
        return jnp.dot(a, b, preferred_element_type=F32)

    def in_cgate():
        @pl.loop(0, 2)
        def _(s):
            cbuf[s] = dot(tfull[s], g_in[0].reshape(D, W))

    def in_value():
        @pl.loop(0, 2)
        def _(s):
            f = wide(s)
            inner = dot(tfull[s], g_in[1].reshape(D, W)) * cbuf[s] * (f * f)
            cbuf[s] = causal(inner, mtaps) * f

    def in_bgate():
        @pl.loop(0, 2)
        def _(s):
            gated[s] = (dot(tfull[s], g_in[2].reshape(D, W)) * cbuf[s]).astype(BF)

    def mix_parts(s, unit):
        for cc in (1 - core, core):
            mat = jnp.concatenate([g_mo[0, 4 * place + 2 * cc + j] for place in order for j in range(2)], axis=1)
            term = dot(gated[s], mat)
            for k in range(4):
                piece = term[:, W * k : W * k + W].reshape(2, HALF, W)
                if cc is core:
                    keep[s, k] = piece
                else:
                    sb[8 * s + 2 * k : 8 * s + 2 * k + 2] = piece.astype(BF)
                    unit.part(k)

    def up_first(s, js):
        for j in js:
            if j < 5:
                acc[s, j] = dot(rfull[s, :, 0:1536], g_up[j, 0:12].reshape(1536, W))
            else:
                acc_tail[s] = dot(rfull[s, :, 0:1536], g_ul[0, 0:12].reshape(1536, 128))

    def tokens_of(s):
        return slice(SEQ * s, SEQ * s + SEQ)

    def silu(v):
        return v / (1.0 + jnp.exp(-v))

    def up_second(s):
        for j in range(5):
            cols = slice(128 * j, 128 * j + 128)
            pre = (acc[s, j] + dot(rfull[s, :, 1536:2048], g_up[j, 12:16].reshape(512, W))) * wide(s)
            taps = jnp.concatenate([ftaps[:, 0, cols], ftaps[:, 1, cols]], axis=1)
            conv = causal(pre, taps)
            active[cols, tokens_of(s)] = (silu(conv[:, 0:128]) * conv[:, 128:256]).T.astype(BF)
        pre = (acc_tail[s] + dot(rfull[s, :, 1536:2048], g_ul[0, 12:16].reshape(512, 128))) * fac[s]
        taps = jnp.concatenate([ftaps[:, 0, tail], ftaps[:, 1, tail]], axis=1)
        conv = causal(pre, taps)
        act = (silu(conv) * pltpu.roll(conv, 64, 1)).T[0:64].astype(BF)
        active[640:704, tokens_of(s)] = act
        active[832:896, tokens_of(s)] = act
        active[704:832, tokens_of(s)] = jnp.zeros((128, SEQ), BF)

    def down_parts(h, unit, cc):
        lo = 640 + 128 * h
        acts = jnp.concatenate([active[0:640, :], active[lo : lo + 128, :]], axis=0)
        mat = jnp.concatenate(
            [
                jnp.concatenate(
                    [g_d[h, 4 * place + 2 * cc + j], g_dt[0, 4 * place + 2 * cc + j]], axis=1
                )
                for place in order
                for j in range(2)
            ],
            axis=0,
        )
        term = dot(mat, acts).reshape(8, 64, 2 * SEQ)
        if cc is core:
            keep2[h] = term
        else:
            sb2[8 * h : 8 * h + 8] = term.astype(BF)
            for k in range(4):
                unit.part(k)

    own = cols_of(1, core)

    pack(0)
    ready("tok")
    pl.semaphore_wait(barrier, 7)
    s1(0)
    for s in range(2):
        gather_own(s, tfull, s)
    s1(1)
    s1(2)
    s2(0)
    s2(1)
    s3(0)
    gather_near(0, tfull, 0)
    tick(1)
    gather_near(1, tfull, 1)
    gather_far(0, tfull, 0)
    near_done(0, tfull, 0)
    add_squares(tfull, 0, (0, 3))
    tick(2)
    gather_far(1, tfull, 1)
    ready("mtaps", "ftaps")
    ahead(3)
    near_done(1, tfull, 1)
    add_squares(tfull, 1, (0, 3))
    for s in range(2):
        far_done(s, tfull, s)
        add_squares(tfull, s, (3, 4))
        row_factor(s)
    done(0)
    in_cgate()
    s4(2)
    ahead(4)
    done(1)
    in_value()
    s4(3)
    done(2)
    in_bgate()
    ahead(5)
    done(3)
    u0, u1 = mix_unit(0), mix_unit(1)
    mix_parts(0, u0)
    s4(4)
    s1(8)
    s2(7)
    u0.far()
    u0.near()
    s3(6)
    mix_parts(1, u1)
    s4(5)
    s1(9)
    s1(10)
    u1.far()
    s2(8)
    u0.last()
    u1.near()
    s3(7)
    s4(6)
    s1(11)
    s2(9)
    u1.last()
    s3(8)
    s2(10)

    def residual(s, unit):
        unit.landed()
        for d in range(2):
            rows = slice(HALF * d, HALF * d + HALF)
            rfull[s, rows, own] = (tfull[s, rows, own].astype(F32) + unit.total(d)).astype(BF)
        gather_own(2 + s, rfull, s)

    residual(0, u0)
    s4(7)
    s1(12)
    residual(1, u1)
    s3(9)
    s2(11)
    s3(10)
    gather_near(2, rfull, 0)
    s4(8)
    near_done(2, rfull, 0)
    add_squares(rfull, 0, (0, 3))
    for r in range(4, 8):
        done(r)
    s4(9)
    s2(12)
    up_first(0, (0, 1, 2, 3))
    s3(11)
    gather_near(3, rfull, 1)
    s4(10)
    done(8)
    done(9)
    up_first(0, (4, 5))
    gather_far(2, rfull, 0)
    s3(12)
    near_done(3, rfull, 1)
    add_squares(rfull, 1, (0, 3))
    up_first(1, (0, 1, 2, 3, 4, 5))
    s4(11)
    gather_far(3, rfull, 1)

    def finish(s):
        far_done(2 + s, rfull, s)
        add_squares(rfull, s, (3, 4))
        row_factor(s)
        up_second(s)

    finish(0)
    finish(1)
    s4(12)
    done(10)
    done(11)
    v0, v1 = ffn_unit(0), ffn_unit(1)
    other = 1 - core
    down_parts(0, v0, other)
    down_parts(0, v0, core)
    v0.far()
    v0.near()
    done(12)
    down_parts(1, v1, other)
    down_parts(1, v1, core)
    v1.far()
    v0.last()
    v1.near()
    v1.last()
    for src, ssem in sent:
        arrived(src, ssem)
    total = []
    for h, unit in enumerate((v0, v1)):
        unit.landed()
        total.append([unit.total(d) for d in range(2)])
    for s in range(2):
        for d in range(2):
            lanes = slice(SEQ * s, SEQ * s + SEQ)
            turned = jnp.concatenate([total[0][d][:, lanes], total[1][d][:, lanes]], axis=0).T
            cols = pl.ds(pl.multiple_of((2 + core) * W + 128 * d, 128), 128)
            out[s, :, 128 * d : 128 * d + 128] = (rfull[s, :, cols].astype(F32) + turned).astype(BF)


def on_device(
    tokens, mix_gain, w_bgate, w_cgate, w_value, in_scale, mix_taps, w_mixout, mixout_scale,
    ffn_gain, w_upgate, w_upval, up_scale, ffn_taps, w_down, down_scale,
):
    args = (
        tokens, mix_gain.reshape(16, 128), w_bgate, w_cgate, w_value, in_scale, mix_taps, w_mixout,
        mixout_scale, ffn_gain.reshape(16, 128), w_upgate.T, w_upval.T, up_scale,
        jnp.swapaxes(ffn_taps, 0, 1), w_down, down_scale,
    )
    vmem = pltpu.VMEM

    def exchange_buffers(piece, kept):
        return (
            vmem((16, *piece), BF),
            vmem((16, *piece), BF),
            vmem((2, *kept, *piece), F32),
            vmem((2, 2, *piece), BF),
            vmem((2, 2, 2, *piece), BF),
            vmem((2, 2, *piece), BF),
            vmem((2, 2, 2, *piece), BF),
        )

    dma = pltpu.SemaphoreType.DMA
    return pl.pallas_call(
        kernel,
        out_shape=vmem(tokens.shape, BF),
        in_specs=[pl.BlockSpec(memory_space=pl.ANY)] * len(args),
        out_specs=pl.BlockSpec(memory_space=pltpu.VMEM),
        scratch_shapes=[
            *(vmem(a.shape, a.dtype) for a in args[1:]),
            vmem((3, 16, 128, W), BF),
            vmem((1, 16, 256, 128), BF),
            vmem((5, 16, 128, W), BF),
            vmem((1, 16, 128, 128), BF),
            vmem((1, 16, 64, 128), BF),
            vmem((2, 16, 64, 640), BF),
            vmem((2, SEQ, D), BF),
            vmem((2, SEQ, D), BF),
            vmem((2, SEQ, W), F32),
            vmem((2, SEQ, W), BF),
            vmem((896, 2 * SEQ), BF),
            vmem((2, SEQ, 128), F32),
            vmem((2, SEQ, 128), F32),
            vmem((2, 5, SEQ, W), F32),
            vmem((2, SEQ, 128), F32),
            *exchange_buffers((HALF, W), (4, 2)),
            *exchange_buffers((64, 2 * SEQ), (8,)),
            dma((ROUNDS,)),
            dma((ROUNDS, 4)),
            dma((4,)),
            dma((4, 5)),
            dma((4,)),
            dma((4, 4)),
            dma((16,)),
        ],
        compiler_params=pltpu.CompilerParams(
            collective_id=0, has_side_effects=True, vmem_limit_bytes=60 * 1024 * 1024
        ),
        name="layer",
    )(*args)


def solution(mesh):
    return jax.shard_map(
        on_device,
        mesh=mesh,
        in_specs=(
            P("fs", None, "tp"),
            P(),
            P("fs", "tp"),
            P("fs", "tp"),
            P("fs", "tp"),
            P(None, "tp"),
            P(None, "tp"),
            P("tp", "fs"),
            P(None, "fs"),
            P(),
            P("fs", "tp"),
            P("fs", "tp"),
            P(None, "tp"),
            P(None, None, "tp"),
            P("tp", "fs"),
            P(None, "fs"),
        ),
        out_specs=P("fs", None, "tp"),
        check_vma=False,
    )
```
